32 devices in a mesh: ep: 16 (over z, y, x), tp: 2 (over core).
Axes of the slice: x: 2, y: 2, z: 4, core: 2. Of those that a mesh axis runs over, the one named last changes fastest.
Arguments:
- tokens: bfloat16 [64, 4096], P('ep'), may hold values from -6 to 6
- memory: float32 [64, 8, 256, 512], P('ep', 'tp'), may hold values from -6 to 6
- normalizer: float32 [64, 8, 256], P('ep', 'tp'), may hold values from -6 to 6
- stabilizer: float32 [64, 8], P('ep', 'tp'), may hold values from -4 to 4
- norm_gain: float32 [4096], replicated, may hold values from 0.1 to 1.9
- w_query: bfloat16 [4096, 8, 256], P(None, 'tp', 'ep'), may hold values from -0.09375 to 0.09375
- w_key: bfloat16 [4096, 8, 256], P(None, 'tp', 'ep'), may hold values from -0.09375 to 0.09375
- w_value: bfloat16 [4096, 8, 512], P(None, 'tp', 'ep'), may hold values from -0.09375 to 0.09375
- w_outgate: bfloat16 [4096, 8, 512], P(None, 'tp', 'ep'), may hold values from -0.09375 to 0.09375
- w_input: bfloat16 [4096, 8], P(None, 'tp'), may hold values from -0.09375 to 0.09375
- w_forget: bfloat16 [4096, 8], P(None, 'tp'), may hold values from -0.09375 to 0.09375
- forget_bias: float32 [8], P('tp'), may hold values from 0 to 4
- w_out: bfloat16 [4096, 4096], P('tp', 'ep'), may hold values from -0.09375 to 0.09375
- ffn_gain: float32 [4096], replicated, may hold values from 0.1 to 1.9
- w_gate: bfloat16 [16, 4096, 512], P('ep', None, 'tp'), may hold values from -0.09375 to 0.09375
- w_up: bfloat16 [16, 4096, 512], P('ep', None, 'tp'), may hold values from -0.09375 to 0.09375
- w_down: bfloat16 [16, 512, 4096], P('ep', 'tp'), may hold values from -0.25 to 0.25
- expert_ids: int32 [64, 2], P('ep'), may hold values from 0 to 15, as said below
- route_weights: float32 [64, 2], P('ep'), may hold values from 0.1 to 1
Outputs:
- out: bfloat16 [64, 4096], P('ep')
- memory_next: float32 [64, 8, 256, 512], P('ep', 'tp')
- normalizer_next: float32 [64, 8, 256], P('ep', 'tp')
- stabilizer_next: float32 [64, 8], P('ep', 'tp')
The draws below stay inside these ranges and needn't reach their ends.
Inputs may be any that keep to these rules, and one draw needn't show every extreme that they name: `expert_ids`: the 2 experts of a token differ and lie in one group of 8 consecutive experts. Beyond that, any choice is allowed: for instance, all 4 tokens of one index of ep may name the same expert.
All inputs are finite; a program needn't handle non-finite values.
Results may differ from the reference program's by a relative error of at most 0.013.
Values may be sent and summed in bfloat16 or wider, within the bound.
No kernel may reach another device: no remote copies, remote signals or barrier semaphores. Data moves between devices by JAX's collectives and lax.ppermute only.
A program may use at most 128 MiB of HBM per device.

```python
import jax
import jax.numpy as jnp
from jax import lax

D = 4096
HEADS = 8
DK = 256
DV = 512
DFF = 512
EXPERTS_PER_GROUP = 8
TOP = 2
SEQ_DEV = 4
SEQS = 64
EXPERTS = 16
GROUPS = 2
N_TP = 2


def draw_expert_ids(key, part):
    keys = jax.random.split(jax.random.fold_in(key, 7), 5)
    owner = jnp.arange(SEQS) // SEQ_DEV
    groups = jnp.minimum(jax.random.randint(keys[0], (SEQS,), 0, GROUPS), jax.random.randint(keys[1], (SEQS,), 0, GROUPS))
    first = jax.random.randint(keys[2], (SEQS,), 0, EXPERTS_PER_GROUP)
    offset = jax.random.randint(keys[3], (SEQS,), 1, EXPERTS_PER_GROUP)
    chosen = jax.random.randint(keys[4], (), 0, SEQS // SEQ_DEV)
    leader = chosen * SEQ_DEV
    groups = jnp.where(owner == chosen, groups[leader], groups)
    first = jnp.where(owner == chosen, first[leader], first)
    second = (first + offset) % EXPERTS_PER_GROUP
    return jnp.stack([groups * EXPERTS_PER_GROUP + first, groups * EXPERTS_PER_GROUP + second], axis=1).astype(jnp.int32)


def level_of(stream_key, shape, shards, least, high):
    def one(axis_at, blocks):
        heights = jax.random.uniform(jax.random.fold_in(jax.random.fold_in(stream_key, 6), axis_at), (blocks,), jnp.float32, least / len(shards), high / len(shards))
        return jnp.repeat(jnp.exp(heights), shape[axis_at] // blocks).reshape((-1,) + (1,) * (len(shape) - axis_at - 1))

    factor_of = one(*shards[0])
    for cut in shards[1:]:
        factor_of = factor_of * one(*cut)
    return factor_of


def gaussian(stream_key, shape, scale, most, cuts=(), held_as=jnp.bfloat16):
    entries = scale * jax.random.normal(stream_key, shape, jnp.float32)
    if cuts:
        entries = entries * level_of(stream_key, shape, cuts, -0.22, 0.18)
    return jnp.clip(entries, -most, most).astype(held_as)


def setup_inputs(seed: int = 0) -> dict:
    arg_keys = jax.random.split(jax.random.key(seed), 20)
    return {
        "tokens": gaussian(arg_keys[0], (SEQS, D), 1.0, 6.0, ((0, 16),)),
        "memory": gaussian(arg_keys[1], (SEQS, HEADS, DK, DV), 1.0, 6.0, ((0, 16), (1, 2)), jnp.float32),
        "normalizer": gaussian(arg_keys[2], (SEQS, HEADS, DK), 1.0, 6.0, ((0, 16), (1, 2)), jnp.float32),
        "stabilizer": gaussian(arg_keys[3], (SEQS, HEADS), 1.0, 4.0, ((0, 16), (1, 2)), jnp.float32),
        "norm_gain": jnp.clip(1.0 + 0.18 * jax.random.normal(arg_keys[4], (D,), jnp.float32), 0.1, 1.9),
        "w_query": gaussian(arg_keys[5], (D, HEADS, DK), D ** -0.5, 0.09375, ((1, 2), (2, 16))),
        "w_key": gaussian(arg_keys[6], (D, HEADS, DK), D ** -0.5, 0.09375, ((1, 2), (2, 16))),
        "w_value": gaussian(arg_keys[7], (D, HEADS, DV), D ** -0.5, 0.09375, ((1, 2), (2, 16))),
        "w_outgate": gaussian(arg_keys[8], (D, HEADS, DV), D ** -0.5, 0.09375, ((1, 2), (2, 16))),
        "w_input": gaussian(arg_keys[9], (D, HEADS), D ** -0.5, 0.09375, ((1, 2),)),
        "w_forget": gaussian(arg_keys[10], (D, HEADS), D ** -0.5, 0.09375, ((1, 2),)),
        "forget_bias": jnp.clip(4.0 * jax.random.uniform(arg_keys[11], (HEADS,), jnp.float32) ** level_of(arg_keys[11], (HEADS,), ((0, 2),), -0.2, 0.2), 0.0, 4.0),
        "w_out": gaussian(arg_keys[12], (HEADS * DV, D), (HEADS * DV) ** -0.5, 0.09375, ((0, 2), (1, 16))),
        "ffn_gain": jnp.clip(1.0 + 0.18 * jax.random.normal(arg_keys[13], (D,), jnp.float32), 0.1, 1.9),
        "w_gate": gaussian(arg_keys[14], (EXPERTS, D, DFF), D ** -0.5, 0.09375, ((0, 16), (2, 2))),
        "w_up": gaussian(arg_keys[15], (EXPERTS, D, DFF), D ** -0.5, 0.09375, ((0, 16), (2, 2))),
        "w_down": gaussian(arg_keys[16], (EXPERTS, DFF, D), DFF ** -0.5, 0.25, ((0, 16), (1, 2))),
        "expert_ids": draw_expert_ids(jax.random.fold_in(arg_keys[19], 71), 0),
        "route_weights": jnp.clip(0.1 + 0.9 * jax.random.uniform(arg_keys[18], (SEQS, TOP), jnp.float32) ** level_of(arg_keys[18], (SEQS, TOP), ((0, 16),), -0.2, 0.2), 0.1, 1.0),
    }


def rms_scale(values, gain):
    return values * lax.rsqrt(lax.optimization_barrier(jnp.mean(values * values, axis=-1, keepdims=True)) + 1e-06) * gain

def product(left, right):
    return jnp.dot(left, right, preferred_element_type=jnp.float32)

def rounded_term(values):
    return lax.optimization_barrier(values.astype(jnp.bfloat16)).astype(jnp.float32)

def cell_step(inputs):
    memory, normalizer, stabilizer, scaled, key, value, in_pre, log_forget = inputs
    stab_next = jnp.maximum(log_forget + stabilizer, in_pre)
    decay = jnp.exp(log_forget + stabilizer - stab_next)
    inweight = jnp.exp(in_pre - stab_next)
    memory_next = decay[:, None, None] * memory + inweight[:, None, None] * (key[:, :, None] * value[:, None, :])
    normalizer_next = decay[:, None] * normalizer + inweight[:, None] * key
    numerator = jnp.einsum('hd,hde->he', scaled, memory_next, precision=lax.Precision.HIGHEST)
    denominator = lax.optimization_barrier(jnp.sum(scaled * normalizer_next, axis=-1))
    hidden = numerator / jnp.maximum(jnp.abs(denominator), jnp.exp(-stab_next))[:, None]
    return (memory_next, normalizer_next, stab_next, hidden)

def reference(tokens, memory, normalizer, stabilizer, norm_gain, w_query, w_key, w_value, w_outgate, w_input, w_forget, forget_bias, w_out, ffn_gain, w_gate, w_up, w_down, expert_ids, route_weights):
    seqs = tokens.shape[0]
    normed = rms_scale(tokens.astype(jnp.float32), norm_gain).astype(jnp.bfloat16)
    query = product(normed, w_query.reshape(D, HEADS * DK)).astype(jnp.bfloat16)
    key = product(normed, w_key.reshape(D, HEADS * DK)).astype(jnp.bfloat16)
    value = product(normed, w_value.reshape(D, HEADS * DV)).astype(jnp.bfloat16)
    outgate = product(normed, w_outgate.reshape(D, HEADS * DV)).astype(jnp.bfloat16)
    in_pre = product(normed, w_input)
    log_forget = jax.nn.log_sigmoid(product(normed, w_forget) + forget_bias)
    scaled = query.astype(jnp.float32).reshape(seqs, HEADS, DK) * DK ** (-0.5)
    key_heads = key.astype(jnp.float32).reshape(seqs, HEADS, DK)
    value_heads = value.astype(jnp.float32).reshape(seqs, HEADS, DV)
    memory_next, normalizer_next, stab_next, hidden = lax.map(cell_step, (memory, normalizer, stabilizer, scaled, key_heads, value_heads, in_pre, log_forget))
    hidden = (hidden.reshape(seqs, HEADS * DV) * jax.nn.sigmoid(outgate.astype(jnp.float32))).astype(jnp.bfloat16)
    span = HEADS * DV // N_TP
    mixed = jnp.zeros((seqs, D), jnp.float32)
    for member in range(N_TP):
        mixed = mixed + rounded_term(product(hidden[:, member * span:(member + 1) * span], w_out[member * span:(member + 1) * span]))
    mixed = mixed.astype(jnp.bfloat16)
    resid = tokens.astype(jnp.float32) + mixed.astype(jnp.float32)
    ffn_in = rms_scale(resid, ffn_gain).astype(jnp.bfloat16)
    hidden_span = DFF // N_TP

    def expert_row(inputs):
        row, expert, weight = inputs
        gate_part = product(row, w_gate[expert])
        up_part = product(row, w_up[expert])
        act = (jax.nn.silu(gate_part) * up_part).astype(jnp.bfloat16)
        down = w_down[expert]
        total = jnp.zeros((D,), jnp.float32)
        for member in range(N_TP):
            total = total + weight * rounded_term(product(act[member * hidden_span:(member + 1) * hidden_span], down[member * hidden_span:(member + 1) * hidden_span]))
        return total
    rows = jnp.repeat(ffn_in, TOP, axis=0)
    weighted = lax.map(expert_row, (rows, expert_ids.reshape(-1).astype(jnp.int32), route_weights.reshape(-1)))
    ffn_out = lax.optimization_barrier(jnp.sum(weighted.reshape(seqs, TOP, D), axis=1))
    out = (resid + ffn_out).astype(jnp.bfloat16)
    return (out, memory_next, normalizer_next, stab_next)
```

```python
import jax
import jax.numpy as jnp
from jax import lax
from jax.sharding import PartitionSpec as P


def rms_scale(values, gain):
    return values * lax.rsqrt(jnp.mean(values * values, axis=-1, keepdims=True) + 1e-06) * gain


def product(left, right):
    return jnp.dot(left, right, preferred_element_type=jnp.float32)


def to_all(block, n_ep):
    copies = jnp.broadcast_to(block[None], (n_ep,) + block.shape)
    return lax.all_to_all(copies, "ep", split_axis=0, concat_axis=0, tiled=True)


def body(
    tokens,
    memory,
    normalizer,
    stabilizer,
    norm_gain,
    w_query,
    w_key,
    w_value,
    w_outgate,
    w_input,
    w_forget,
    forget_bias,
    w_out,
    ffn_gain,
    w_gate,
    w_up,
    w_down,
    expert_ids,
    route_weights,
):
    n_ep = lax.axis_size("ep")
    n_tp = lax.axis_size("tp")
    me_ep = lax.axis_index("ep")
    me_tp = lax.axis_index("tp")
    seqs, width = tokens.shape
    share = seqs // n_tp
    heads, key_size, value_size = (memory.shape[1], memory.shape[2], memory.shape[3])
    value_width = heads * value_size
    key_piece = w_query.shape[2]
    value_piece = w_value.shape[2]

    tokens_share = lax.dynamic_slice_in_dim(tokens, me_tp * share, share, 0)
    raw_share = to_all(tokens_share, n_ep).reshape(n_ep * share, width)
    raw_share_f32 = raw_share.astype(jnp.float32)
    normed_share = rms_scale(raw_share_f32, norm_gain).astype(jnp.bfloat16)
    normed_all = lax.all_gather(normed_share, "tp", axis=0, tiled=True)

    columns = [w.reshape(width, -1) for w in (w_query, w_key, w_value, w_outgate)]
    projected = jnp.concatenate([product(normed_all, w) for w in columns], axis=1).astype(jnp.bfloat16)
    total = projected.shape[1]
    projected = jnp.swapaxes(projected.reshape(n_tp, n_ep, share, total), 0, 1)
    projected = projected.reshape(n_ep, seqs, total)
    pieces = lax.all_to_all(projected, "ep", split_axis=0, concat_axis=0, tiled=True)

    def heads_of(start, piece):
        part = pieces[:, :, start : start + heads * piece].reshape(n_ep, seqs, heads, piece)
        return jnp.transpose(part, (1, 2, 0, 3)).reshape(seqs, heads, n_ep * piece).astype(jnp.float32)

    narrow = heads * key_piece
    broad = heads * value_piece
    scaled = heads_of(0, key_piece) * key_size ** (-0.5)
    key_heads = heads_of(narrow, key_piece)
    value_heads = heads_of(2 * narrow, value_piece)
    outgate = heads_of(2 * narrow + broad, value_piece)

    normed = rms_scale(tokens.astype(jnp.float32), norm_gain).astype(jnp.bfloat16)
    in_pre = product(normed, w_input)
    log_forget = jax.nn.log_sigmoid(product(normed, w_forget) + forget_bias)
    stab_next = jnp.maximum(log_forget + stabilizer, in_pre)
    decay = jnp.exp(log_forget + stabilizer - stab_next)
    inweight = jnp.exp(in_pre - stab_next)

    normalizer_next = decay[:, :, None] * normalizer + inweight[:, :, None] * key_heads
    denominator = jnp.sum(scaled * normalizer_next, axis=-1)
    along = jnp.sum(scaled * key_heads, axis=-1)
    recalled = jnp.sum(scaled[:, :, :, None] * memory, axis=2)
    numerator = decay[:, :, None] * recalled + (inweight * along)[:, :, None] * value_heads
    hidden = numerator / jnp.maximum(jnp.abs(denominator), jnp.exp(-stab_next))[:, :, None]
    hidden = (hidden * jax.nn.sigmoid(outgate)).reshape(seqs, value_width).astype(jnp.bfloat16)
    memory_next = decay[:, :, None, None] * memory + inweight[:, :, None, None] * (
        key_heads[:, :, :, None] * value_heads[:, :, None, :]
    )

    hidden_all = to_all(hidden, n_ep).reshape(n_ep * seqs, value_width)
    term = product(hidden_all, w_out).astype(jnp.bfloat16).reshape(n_ep, n_tp, share, -1)
    own_term = lax.dynamic_index_in_dim(term, me_tp, 1, keepdims=False)
    mixed = own_term.astype(jnp.float32)
    for step in range(1, n_tp):
        theirs = lax.dynamic_index_in_dim(term, (me_tp + step) % n_tp, 1, keepdims=False)
        shift = [(i, (i + step) % n_tp) for i in range(n_tp)]
        mixed = mixed + lax.ppermute(theirs, "tp", shift).astype(jnp.float32)
    mixed = mixed.astype(jnp.bfloat16).reshape(n_ep * share, -1)
    mixed_share = jnp.swapaxes(to_all(mixed, n_ep), 0, 1).reshape(n_ep * share, width)

    resid_share = raw_share_f32 + mixed_share.astype(jnp.float32)
    ffn_share = rms_scale(resid_share, ffn_gain).astype(jnp.bfloat16)
    ffn_all = lax.all_gather(ffn_share, "tp", axis=0, tiled=True)

    gate_part = product(ffn_all, w_gate[0])
    up_part = product(ffn_all, w_up[0])
    act = (jax.nn.silu(gate_part) * up_part).astype(jnp.bfloat16)
    down_term = product(act, w_down[0]).astype(jnp.bfloat16).reshape(n_tp, n_ep * share, width)
    summed = lax.dynamic_index_in_dim(down_term, me_tp, 0, keepdims=False).astype(jnp.float32)
    for step in range(1, n_tp):
        theirs = lax.dynamic_index_in_dim(down_term, (me_tp + step) % n_tp, 0, keepdims=False)
        shift = [(i, (i + step) % n_tp) for i in range(n_tp)]
        summed = summed + lax.ppermute(theirs, "tp", shift).astype(jnp.float32)
    summed = summed.astype(jnp.bfloat16).reshape(n_ep, share, width)
    by_expert = lax.all_to_all(summed, "ep", split_axis=0, concat_axis=0, tiled=True)

    n_experts = n_ep * w_gate.shape[0]
    labels = jnp.arange(n_experts, dtype=jnp.int32)
    ids = lax.dynamic_slice_in_dim(expert_ids, me_tp * share, share, 0)
    gains = lax.dynamic_slice_in_dim(route_weights, me_tp * share, share, 0)
    route = jnp.sum(jnp.where(ids[:, :, None] == labels[None, None, :], gains[:, :, None], 0.0), axis=1)
    ffn_out = jnp.sum(by_expert.astype(jnp.float32) * jnp.swapaxes(route, 0, 1)[:, :, None], axis=0)
    resid_own = lax.dynamic_slice_in_dim(resid_share, me_ep * share, share, 0)
    out_share = (resid_own + ffn_out).astype(jnp.bfloat16)
    out = lax.all_gather(out_share, "tp", axis=0, tiled=True)
    return (out, memory_next, normalizer_next, stab_next)


def solution(mesh):
    return jax.shard_map(
        body,
        mesh=mesh,
        in_specs=(
            P("ep", None),
            P("ep", "tp", None, None),
            P("ep", "tp", None),
            P("ep", "tp"),
            P(),
            P(None, "tp", "ep"),
            P(None, "tp", "ep"),
            P(None, "tp", "ep"),
            P(None, "tp", "ep"),
            P(None, "tp"),
            P(None, "tp"),
            P("tp"),
            P("tp", "ep"),
            P(),
            P("ep", None, "tp"),
            P("ep", None, "tp"),
            P("ep", "tp", None),
            P("ep", None),
            P("ep", None),
        ),
        out_specs=(P("ep", None), P("ep", "tp", None, None), P("ep", "tp", None), P("ep", "tp")),
        check_vma=False,
    )
```

```python
import functools

import jax
import jax.numpy as jnp
from jax import lax
from jax.experimental import pallas as pl
from jax.experimental.pallas import tpu as pltpu
from jax.sharding import PartitionSpec as P

F32 = jnp.float32
BF16 = jnp.bfloat16
ANY = pl.BlockSpec(memory_space=pl.ANY)
HBM = pl.BlockSpec(memory_space=pltpu.HBM)
VMEM = pl.BlockSpec(memory_space=pltpu.VMEM)


def rms_scale(values, gain):
    return values * lax.rsqrt(jnp.mean(values * values, axis=-1, keepdims=True) + 1e-06) * gain


def product(left, right):
    return jnp.dot(left, right, preferred_element_type=F32)


def product_t(left, right):
    return lax.dot_general(left, right, (((1,), (1,)), ((), ())), preferred_element_type=F32)


def to_all(copies):
    return lax.all_to_all(copies, "ep", split_axis=0, concat_axis=0, tiled=True)


def call(kernel, out_shape, in_specs, scratch, args, name, kib=24576, flops=10**6, nbytes=10**6, outs=None):
    many = isinstance(out_shape, tuple)
    args = [pltpu.with_memory_space_constraint(a, pltpu.HBM) if s is HBM else a for a, s in zip(args, in_specs)]
    return pl.pallas_call(
        kernel,
        out_shape=out_shape,
        in_specs=in_specs,
        out_specs=outs or (tuple(VMEM for _ in out_shape) if many else VMEM),
        scratch_shapes=scratch,
        name=name,
        compiler_params=pltpu.CompilerParams(vmem_limit_bytes=kib << 10),
        cost_estimate=pl.CostEstimate(flops=flops, transcendentals=0, bytes_accessed=nbytes),
    )(*args)


def shape(dims, dtype):
    return jax.ShapeDtypeStruct(dims, dtype)


def project_kernel(own, other, gain, wq, wk, wv, wo, out, weights, normed, sems, *, seqs):
    starts, copies = 0, []
    for n, w in enumerate((wq, wk, wv, wo)):
        rows = w.shape[0]
        copies.append(pltpu.make_async_copy(w, weights.at[pl.ds(starts, rows)], sems.at[n]))
        copies[-1].start()
        starts += rows
    half = own.shape[0]
    scale = gain[...]
    normed[0:half] = rms_scale(own[...].astype(F32), scale).astype(BF16)
    normed[half:] = rms_scale(other[...].astype(F32), scale).astype(BF16)
    front = starts - wo.shape[0]
    for c in copies[:3]:
        c.wait()
    left = product_t(normed[...], weights[0:front]).astype(BF16)
    copies[3].wait()
    right = product_t(normed[...], weights[front:starts]).astype(BF16)
    rows = 2 * half
    share = seqs // 2
    me = lax.axis_index("tp")
    r = lax.broadcasted_iota(jnp.int32, (rows, rows), 0)
    c = lax.broadcasted_iota(jnp.int32, (rows, rows), 1)
    token = r % seqs
    which = (token // share + me) % 2
    pick = (c == which * half + (r // seqs) * share + token % share).astype(BF16)
    left = product(pick, left)
    right = product(pick, right)
    for d in range(rows // seqs):
        out[d, :, 0:front] = left[d * seqs : (d + 1) * seqs].astype(BF16)
        out[d, :, front:starts] = right[d * seqs : (d + 1) * seqs].astype(BF16)


def readout_kernel(query, key, value, outgate, decay, inweight, floor, norm, memory, out, norm_out, buf, recalled, sems):
    seqs, heads, dk, dv = memory.shape
    copies = []
    for i in range(seqs):
        for h in range(heads):
            n = i * heads + h
            copies.append(pltpu.make_async_copy(memory.at[i, h], buf.at[n], sems.at[n]))
            copies[-1].start()
    columns = query[...].T
    for n, c in enumerate(copies):
        c.wait()
        i, h = divmod(n, heads)
        part = jnp.sum(buf[n] * columns[:, n : n + 1], axis=0, keepdims=True)
        recalled[i : i + 1, h * dv : (h + 1) * dv] = part
    for h in range(heads):
        rows = [i * heads + h for i in range(seqs)]
        q = jnp.concatenate([query[n : n + 1] for n in rows], axis=0)
        k = jnp.concatenate([key[n : n + 1] for n in rows], axis=0)
        old = jnp.concatenate([norm[n : n + 1] for n in rows], axis=0)
        d = decay[:, h : h + 1]
        w = inweight[:, h : h + 1]
        new = d * old + w * k
        for i, n in enumerate(rows):
            norm_out[n : n + 1] = new[i : i + 1]
        below = jnp.maximum(jnp.abs(jnp.sum(q * new, axis=1, keepdims=True)), floor[:, h : h + 1])
        along = w * jnp.sum(q * k, axis=1, keepdims=True)
        at = slice(h * dv, (h + 1) * dv)
        top = d * recalled[:, at] + along * value[:, at]
        hidden = (top / below * jax.nn.sigmoid(outgate[:, at])).astype(BF16)
        for e in range(out.shape[0]):
            out[e, :, at] = hidden


def update_kernel(key, value, decay, inweight, after, memory, out, token, buf, sems, out_sems):
    token[...] = jnp.zeros(token.shape, F32)
    seqs, heads, dk, dv = memory.shape
    copies, backs = [], []
    for i in range(seqs):
        for h in range(heads):
            n = i * heads + h
            copies.append(pltpu.make_async_copy(memory.at[i, h], buf.at[n], sems.at[n]))
            copies[-1].start()
    columns = key[...].T
    for n, c in enumerate(copies):
        c.wait()
        i, h = divmod(n, heads)
        d = decay[i : i + 1, h : h + 1]
        w = inweight[i : i + 1, h : h + 1]
        row = value[i : i + 1, h * dv : (h + 1) * dv] * w
        buf[n] = d * buf[n] + columns[:, n : n + 1] * row
        backs.append(pltpu.make_async_copy(buf.at[n], out.at[i, h], out_sems.at[n]))
        backs[-1].start()
    for b in backs:
        b.wait()


def output_kernel(hidden, token, w_out, own, other, weights, sems, *, seqs):
    parts = sems.shape[0]
    rows = w_out.shape[0] // parts
    copies = []
    for n in range(parts):
        at = pl.ds(n * rows, rows)
        copies.append(pltpu.make_async_copy(w_out.at[at], weights.at[at], sems.at[n]))
        copies[-1].start()
    total = None
    for n, c in enumerate(copies):
        c.wait()
        part = product(hidden[:, n * rows : (n + 1) * rows], weights[n * rows : (n + 1) * rows])
        total = part if total is None else total + part
    term = total.astype(BF16)
    half, share = own.shape[0], seqs // 2
    me = lax.axis_index("tp")
    r = lax.broadcasted_iota(jnp.int32, (half, 2 * half), 0)
    c = lax.broadcasted_iota(jnp.int32, (half, 2 * half), 1)
    at = (r // share) * seqs + r % share
    own[...] = product((c == at + me * share).astype(BF16), term).astype(BF16)
    other[...] = product((c == at + (1 - me) * share).astype(BF16), term).astype(BF16)


def resid_kernel(raw, mixed, gain, ffn, mine, resid):
    members, rows, cols = mixed.shape
    group = max(1, 128 // cols)
    total = None
    for n in range(0, members, group):
        part = jnp.concatenate([mixed[n + g] for g in range(group)], axis=1) if group > 1 else mixed[n]
        at = slice(n * cols, (n + group) * cols)
        block = raw[:, at].astype(F32) + part.astype(F32)
        resid[:, at] = block
        squares = jnp.sum(block * block, axis=1, keepdims=True)
        total = squares if total is None else total + squares
    scale = lax.rsqrt(total / (members * cols) + 1e-06)
    ffn[...] = (resid[...] * scale * gain[...]).astype(BF16)
    share = mine.shape[0]
    me = lax.axis_index("ep")
    for j in range(share):
        mine[j : j + 1] = resid[pl.ds(me * share + j, 1)]


def expert_kernel(own, other, w_gate, w_up, w_down, out_own, out_other, gate, up, down, sems):
    parts = sems.shape[1]
    copies = [[], [], []]
    for n in range(parts):
        for k, (w, buf) in enumerate(((w_gate, gate), (w_up, up))):
            rows = w.shape[1] // parts
            at = pl.ds(n * rows, rows)
            copies[k].append(pltpu.make_async_copy(w.at[0, at], buf.at[at], sems.at[k, n]))
            copies[k][-1].start()
    width = w_down.shape[2] // parts
    for n in range(parts):
        at = pl.ds(n * width, width)
        copies[2].append(pltpu.make_async_copy(w_down.at[0, :, at], down.at[:, at], sems.at[2, n]))
        copies[2][-1].start()
    rows = w_gate.shape[1] // parts
    gate_sum = up_sum = None
    for n in range(parts):
        at = slice(n * rows, (n + 1) * rows)
        left = jnp.concatenate([own[:, at], other[:, at]], axis=0)
        copies[0][n].wait()
        part = product(left, gate[at])
        gate_sum = part if gate_sum is None else gate_sum + part
        copies[1][n].wait()
        part = product(left, up[at])
        up_sum = part if up_sum is None else up_sum + part
    act = (jax.nn.silu(gate_sum) * up_sum).astype(BF16)
    half = own.shape[0]
    for n in range(parts):
        at = slice(n * width, (n + 1) * width)
        copies[2][n].wait()
        term = product(act, down[:, at]).astype(BF16)
        out_own[:, at] = term[0:half]
        out_other[:, at] = term[half:]


def join_kernel(own, other, out):
    share = out.shape[1]
    both = own[...].astype(F32) + other[...].astype(F32)
    for e in range(out.shape[0]):
        out[e] = both[e * share : (e + 1) * share].astype(BF16)


def share_kernel(tokens, out):
    share = out.shape[1]
    me = lax.axis_index("tp")
    values = tokens[...].astype(F32)
    mine = jnp.where(me == 0, values[0:share], values[share:]).astype(BF16)
    for e in range(out.shape[0]):
        out[e] = mine


def gates_kernel(tokens, gain, w_in, w_forget, bias, stab, stab_out, decay, inweight, floor):
    normed = rms_scale(tokens[...].astype(F32), gain[...]).astype(BF16)
    in_pre = product_t(normed, w_in[...])
    old = jax.nn.log_sigmoid(product_t(normed, w_forget[...]) + bias[...]) + stab[...]
    new = jnp.maximum(old, in_pre)
    stab_out[...] = new
    decay[...] = jnp.exp(old - new)
    inweight[...] = jnp.exp(in_pre - new)
    floor[...] = jnp.exp(-new)


def body(
    tokens,
    memory,
    normalizer,
    stabilizer,
    norm_gain,
    w_query,
    w_key,
    w_value,
    w_outgate,
    w_input,
    w_forget,
    forget_bias,
    w_out,
    ffn_gain,
    w_gate,
    w_up,
    w_down,
    expert_ids,
    route_weights,
):
    n_ep = lax.axis_size("ep")
    n_tp = lax.axis_size("tp")
    assert n_tp == 2
    me_tp = lax.axis_index("tp")
    swap = [(0, 1), (1, 0)]
    seqs, width = tokens.shape
    share = seqs // n_tp
    half = n_ep * share
    heads, key_size, value_size = (memory.shape[1], memory.shape[2], memory.shape[3])
    value_width = heads * value_size
    key_piece = w_query.shape[2]
    value_piece = w_value.shape[2]
    narrow = heads * key_piece
    broad = heads * value_piece
    total = 2 * narrow + 2 * broad

    copies = call(share_kernel, shape((n_ep, share, width), BF16), [VMEM], [], [tokens], "share")
    raw_own = to_all(copies).reshape(half, width)
    raw_other = lax.ppermute(raw_own, "tp", swap)

    columns = [jnp.transpose(w, (1, 2, 0)).reshape(-1, width) for w in (w_query, w_key, w_value, w_outgate)]
    projected = call(
        functools.partial(project_kernel, seqs=seqs),
        shape((n_ep, seqs, total), BF16),
        [VMEM, VMEM, VMEM, HBM, HBM, HBM, HBM],
        [pltpu.VMEM((total, width), BF16), pltpu.VMEM((2 * half, width), BF16), pltpu.SemaphoreType.DMA((4,))],
        [raw_own, raw_other, norm_gain.reshape(1, width), *columns],
        "project",
        flops=2 * 2 * half * total * width,
    )
    pieces = to_all(projected)

    def rows_of(start, piece):
        part = pieces[:, :, start : start + heads * piece].reshape(n_ep, seqs, heads, piece)
        return jnp.transpose(part, (1, 2, 0, 3)).astype(F32)

    query = (rows_of(0, key_piece) * key_size ** (-0.5)).reshape(seqs * heads, key_size)
    key = rows_of(narrow, key_piece).reshape(seqs * heads, key_size)
    value = rows_of(2 * narrow, value_piece).reshape(seqs, value_width)
    outgate = rows_of(2 * narrow + broad, value_piece).reshape(seqs, value_width)

    stab_next, decay, inweight, floor = call(
        gates_kernel,
        (shape((seqs, heads), F32),) * 4,
        [VMEM] * 6,
        [],
        [tokens, norm_gain.reshape(1, width), w_input.T, w_forget.T, forget_bias.reshape(1, heads), stabilizer],
        "gates",
    )

    n_cells = seqs * heads
    hidden, norm_next = call(
        readout_kernel,
        (shape((n_ep, seqs, value_width), BF16), shape((n_cells, key_size), F32)),
        [VMEM] * 8 + [HBM],
        [
            pltpu.VMEM((n_cells, key_size, value_size), F32),
            pltpu.VMEM((seqs, value_width), F32),
            pltpu.SemaphoreType.DMA((n_cells,)),
        ],
        [query, key, value, outgate, decay, inweight, floor, normalizer.reshape(n_cells, key_size), memory],
        "readout",
        flops=2 * memory.size,
    )
    hidden_all = to_all(hidden).reshape(n_ep * seqs, value_width)
    memory_next, token = call(
        update_kernel,
        (shape(memory.shape, F32), shape((8, 128), F32)),
        [VMEM] * 4 + [ANY, HBM],
        [
            pltpu.VMEM((n_cells, key_size, value_size), F32),
            pltpu.SemaphoreType.DMA((n_cells,)),
            pltpu.SemaphoreType.DMA((n_cells,)),
        ],
        [key, value, decay, inweight, norm_next, memory],
        "update",
        flops=10**8,
        outs=(HBM, VMEM),
    )

    own_term, other_term = call(
        functools.partial(output_kernel, seqs=seqs),
        (shape((half, w_out.shape[1]), BF16),) * 2,
        [VMEM, ANY, HBM],
        [pltpu.VMEM(w_out.shape, BF16), pltpu.SemaphoreType.DMA((4,))],
        [hidden_all, token, w_out],
        "output",
        flops=2 * n_ep * seqs * w_out.size,
    )
    mixed = (own_term.astype(F32) + lax.ppermute(other_term, "tp", swap).astype(F32)).astype(BF16)
    mixed_all = to_all(jnp.broadcast_to(mixed[None], (n_ep,) + mixed.shape))

    ffn_own, resid_mine = call(
        resid_kernel,
        (shape((half, width), BF16), shape((share, width), F32)),
        [VMEM] * 3,
        [pltpu.VMEM((half, width), F32)],
        [raw_own, mixed_all, ffn_gain.reshape(1, width)],
        "resid",
    )
    ffn_other = lax.ppermute(ffn_own, "tp", swap)
    units = w_gate.shape[2]
    down_own, down_other = call(
        expert_kernel,
        (shape((half, width), BF16),) * 2,
        [VMEM, VMEM, HBM, HBM, HBM],
        [
            pltpu.VMEM((width, units), BF16),
            pltpu.VMEM((width, units), BF16),
            pltpu.VMEM((units, width), BF16),
            pltpu.SemaphoreType.DMA((3, 4)),
        ],
        [ffn_own, ffn_other, w_gate, w_up, w_down],
        "experts",
        flops=2 * 3 * 2 * half * width * units,
    )
    summed = call(
        join_kernel,
        shape((n_ep, share, width), BF16),
        [VMEM] * 2,
        [],
        [down_own, lax.ppermute(down_other, "tp", swap)],
        "join",
    )
    by_expert = to_all(summed)

    n_experts = n_ep * w_gate.shape[0]
    labels = jnp.arange(n_experts, dtype=jnp.int32)
    ids = lax.dynamic_slice_in_dim(expert_ids, me_tp * share, share, 0)
    gains = lax.dynamic_slice_in_dim(route_weights, me_tp * share, share, 0)
    route = jnp.sum(jnp.where(ids[:, :, None] == labels[None, None, :], gains[:, :, None], 0.0), axis=1)
    ffn_out = jnp.sum(by_expert.astype(F32) * jnp.swapaxes(route, 0, 1)[:, :, None], axis=0)
    out_mine = (resid_mine + ffn_out).astype(BF16)
    out_other = lax.ppermute(out_mine, "tp", swap)
    first = jnp.where(me_tp == 0, out_mine, out_other)
    last = jnp.where(me_tp == 0, out_other, out_mine)
    out = jnp.concatenate([first, last], axis=0)
    return (out, memory_next, norm_next.reshape(normalizer.shape), stab_next)


def solution(mesh):
    return jax.shard_map(
        body,
        mesh=mesh,
        in_specs=(
            P("ep", None),
            P("ep", "tp", None, None),
            P("ep", "tp", None),
            P("ep", "tp"),
            P(),
            P(None, "tp", "ep"),
            P(None, "tp", "ep"),
            P(None, "tp", "ep"),
            P(None, "tp", "ep"),
            P(None, "tp"),
            P(None, "tp"),
            P("tp"),
            P("tp", "ep"),
            P(),
            P("ep", None, "tp"),
            P("ep", None, "tp"),
            P("ep", "tp", None),
            P("ep", None),
            P("ep", None),
        ),
        out_specs=(P("ep", None), P("ep", "tp", None, None), P("ep", "tp", None), P("ep", "tp")),
        check_vma=False,
    )
```

```python
import functools

import jax
import jax.numpy as jnp
from jax import lax
from jax.experimental import pallas as pl
from jax.experimental.pallas import tpu as pltpu
from jax.sharding import PartitionSpec as P

F32 = jnp.float32
BF16 = jnp.bfloat16
ANY = pl.BlockSpec(memory_space=pl.ANY)
HBM = pl.BlockSpec(memory_space=pltpu.HBM)
VMEM = pl.BlockSpec(memory_space=pltpu.VMEM)
FAST = pl.BlockSpec(memory_space=pltpu.VMEM)


def rms_scale(values, gain):
    return values * lax.rsqrt(jnp.mean(values * values, axis=-1, keepdims=True) + 1e-06) * gain


def product(left, right):
    return jnp.dot(left, right, preferred_element_type=F32)


def product_t(left, right):
    return lax.dot_general(left, right, (((1,), (1,)), ((), ())), preferred_element_type=F32)


def to_all(copies):
    return lax.all_to_all(copies, "ep", split_axis=0, concat_axis=0, tiled=True)


def call(kernel, out_shape, in_specs, scratch, args, name, flops=10**6, outs=None):
    many = isinstance(out_shape, tuple)
    outs = outs or (tuple(VMEM for _ in out_shape) if many else VMEM)
    pins = {id(HBM): pltpu.HBM, id(FAST): pltpu.VMEM}
    args = [pltpu.with_memory_space_constraint(a, pins[id(s)]) if id(s) in pins else a for a, s in zip(args, in_specs)]
    return pl.pallas_call(
        kernel,
        out_shape=out_shape,
        in_specs=in_specs,
        out_specs=outs,
        scratch_shapes=scratch,
        name=name,
        compiler_params=pltpu.CompilerParams(vmem_limit_bytes=24 << 20),
        cost_estimate=pl.CostEstimate(flops=flops, transcendentals=0, bytes_accessed=10**6),
    )(*args)


def shape(dims, dtype):
    return jax.ShapeDtypeStruct(dims, dtype)


def fetch(pairs, sems):
    copies = [pltpu.make_async_copy(src, dst, sems.at[n]) for n, (src, dst) in enumerate(pairs)]
    for c in copies:
        c.start()
    return copies


def front_kernel(own, gain, wq, wk, wv, gain_out, weights, normed, sems):
    pairs, at = [(gain, gain_out)], 0
    for w in (wq, wk, wv):
        pairs.append((w, weights.at[pl.ds(at, w.shape[0])]))
        at += w.shape[0]
    copies = fetch(pairs, sems)
    copies[0].wait()
    normed[...] = rms_scale(own[...].astype(F32), gain_out[...]).astype(BF16)
    for c in copies[1:]:
        c.wait()


def recall_kernel(after, memory, out, sems):
    heads = memory.shape[1]
    for c in fetch([(memory.at[n // heads, n % heads], out.at[n]) for n in range(out.shape[0])], sems):
        c.wait()


def units_kernel(after, w_gate, w_up, out, sems):
    rows, units = out.shape[0] // 2, out.shape[1] // 2
    pairs = []
    for n in range(2):
        at = pl.ds(n * rows, rows)
        pairs.append((w_gate.at[0, at], out.at[at, pl.ds(0, units)]))
        pairs.append((w_up.at[0, at], out.at[at, pl.ds(units, units)]))
    for c in fetch(pairs, sems):
        c.wait()


def expert_kernel(own, other, near, w_gate, w_up, w_down, act_own, down, out, far, sems, down_sems):
    done, units = near.shape[0], w_gate.shape[2]
    parts = sems.shape[0] // 2
    rows = far.shape[0] // parts
    pairs = []
    for n in range(parts):
        src, dst = pl.ds(done + n * rows, rows), pl.ds(n * rows, rows)
        pairs.append((w_gate.at[0, src], far.at[dst, pl.ds(0, units)]))
        pairs.append((w_up.at[0, src], far.at[dst, pl.ds(units, units)]))
    copies = fetch(pairs, sems)
    slabs = down_sems.shape[0]
    width = w_down.shape[2] // slabs
    at = [pl.ds(n * width, width) for n in range(slabs)]
    downs = fetch([(w_down.at[0, :, a], down.at[:, a]) for a in at], down_sems)

    def left(start, stop):
        return jnp.concatenate([own[:, start:stop], other[:, start:stop]], axis=0)

    total = product(left(0, done), near[...])
    for n in range(parts):
        copies[2 * n].wait()
        copies[2 * n + 1].wait()
        start = done + n * rows
        total = total + product(left(start, start + rows), far[n * rows : (n + 1) * rows])
    act = (jax.nn.silu(total[:, 0:units]) * total[:, units:]).astype(BF16)
    half = own.shape[0]
    act_own[...] = act[0:half]
    for n in range(slabs):
        downs[n].wait()
        at = slice(n * width, (n + 1) * width)
        out[:, at] = product(act[half:], down[:, at]).astype(BF16)


def down_kernel(act, down, out):
    out[...] = product(act[...], down[...]).astype(BF16)


def project_kernel(own, other, gain, front, wo, out, back, normed, sems, *, seqs):
    (copy,) = fetch([(wo, back)], sems)
    half = other.shape[0]
    normed[0:half] = own[...]
    normed[half:] = rms_scale(other[...].astype(F32), gain[...]).astype(BF16)
    left = product_t(front[...], normed[...]).astype(BF16)
    copy.wait()
    right = product_t(back[...], normed[...]).astype(BF16)
    rows = 2 * half
    share = seqs // 2
    me = lax.axis_index("tp")
    r = lax.broadcasted_iota(jnp.int32, (rows, rows), 0)
    c = lax.broadcasted_iota(jnp.int32, (rows, rows), 1)
    token = r % seqs
    which = (token // share + me) % 2
    pick = (c == which * half + (r // seqs) * share + token % share).astype(BF16)
    left = product_t(pick, left)
    right = product_t(pick, right)
    cut = front.shape[0]
    for d in range(rows // seqs):
        out[d, :, 0:cut] = left[d * seqs : (d + 1) * seqs].astype(BF16)
        out[d, :, cut:] = right[d * seqs : (d + 1) * seqs].astype(BF16)


def spread(pieces, start, piece, blocks, seqs):
    rows, total = pieces.shape
    members = rows // seqs
    low = start // 128 * 128
    high = min(total, -(-(start + blocks * piece) // 128) * 128)
    entries = members * piece
    wide = blocks * entries
    d = lax.broadcasted_iota(jnp.int32, (1, wide), 1)
    target = start - low + (d // entries) * piece + d % piece
    column = lax.broadcasted_iota(jnp.int32, (high - low, wide), 0)
    placed = product(pieces[:, low:high], jnp.where(column == target, 1.0, 0.0).astype(BF16))
    member = (d % entries) // piece
    r = lax.broadcasted_iota(jnp.int32, (rows, wide), 0) // seqs
    placed = jnp.where(r == member, placed, 0.0).astype(BF16)
    t = lax.broadcasted_iota(jnp.int32, (8, rows), 0)
    gather = jnp.where(lax.broadcasted_iota(jnp.int32, (8, rows), 1) % seqs == t, 1.0, 0.0)
    return product(gather.astype(BF16), placed)


def readout_kernel(
    pieces,
    decay,
    inweight,
    floor,
    norm,
    first,
    memory,
    out,
    norm_out,
    key_out,
    value_out,
    buf,
    recalled,
    hidden,
    sems,
    out_sems,
    *,
    piece,
):
    seqs, heads, dk, dv = memory.shape
    near = first.shape[0]
    cells = [(n // heads, n % heads) for n in range(seqs * heads)]
    copies = fetch([(memory.at[i, h], buf.at[n]) for n, (i, h) in enumerate(cells[near:])], sems)
    rows = jnp.concatenate([pieces[m].astype(F32) for m in range(pieces.shape[0])], axis=0).astype(BF16)
    small, large = piece
    narrow = spread(rows, 0, small, 2 * heads, seqs)
    key_at = heads * dk
    query = [narrow[:, h * dk : (h + 1) * dk] * dk ** (-0.5) for h in range(heads)]
    key = [narrow[:, key_at + h * dk : key_at + (h + 1) * dk] for h in range(heads)]
    columns = jnp.concatenate(query, axis=0).T

    def recall(cell, i, h):
        n = h * 8 + i
        part = jnp.sum(cell * columns[:, n : n + 1], axis=0, keepdims=True)
        recalled[i : i + 1, h * dv : (h + 1) * dv] = part

    for n, (i, h) in enumerate(cells[:near]):
        recall(first[n], i, h)
    value = spread(rows, 2 * heads * small, large, heads, seqs)[0:seqs]
    outgate = spread(rows, 2 * heads * small + heads * large, large, heads, seqs)[0:seqs]
    value_out[...] = value
    below, along = [], []
    for h in range(heads):
        key_out[h * 8 : (h + 1) * 8] = key[h]
        q, k = query[h][0:seqs], key[h][0:seqs]
        old = jnp.concatenate([norm[i, h : h + 1] for i in range(seqs)], axis=0)
        w = inweight[:, h : h + 1]
        new = decay[:, h : h + 1] * old + w * k
        for i in range(seqs):
            norm_out[i, h : h + 1] = new[i : i + 1]
        below.append(jnp.maximum(jnp.abs(jnp.sum(q * new, axis=1, keepdims=True)), floor[:, h : h + 1]))
        along.append(w * jnp.sum(q * k, axis=1, keepdims=True))
    gate = jax.nn.sigmoid(outgate)
    for n, (i, h) in enumerate(cells[near:]):
        copies[n].wait()
        recall(buf[n], i, h)
    for h in range(heads):
        at = slice(h * dv, (h + 1) * dv)
        top = decay[:, h : h + 1] * recalled[:, at] + along[h] * value[:, at]
        hidden[:, at] = (top / below[h] * gate[:, at]).astype(BF16)
    for c in fetch([(hidden, out.at[e]) for e in range(out.shape[0])], out_sems):
        c.wait()


def update_kernel(key, value, decay, inweight, w_out, memory, out, w_copy, buf, sems, out_sems, w_sems):
    seqs, heads, dk, dv = memory.shape
    cells = [(i, h) for i in range(seqs) for h in range(heads)]
    copies = fetch([(memory.at[i, h], buf.at[n]) for n, (i, h) in enumerate(cells)], sems)
    extra = fetch([(w_out, w_copy)], w_sems)
    backs = []
    columns = key[...].T
    for n, (i, h) in enumerate(cells):
        copies[n].wait()
        d = decay[i : i + 1, h : h + 1]
        row = value[i : i + 1, h * dv : (h + 1) * dv] * inweight[i : i + 1, h : h + 1]
        at = h * 8 + i
        buf[n] = d * buf[n] + columns[:, at : at + 1] * row
        backs.append(pltpu.make_async_copy(buf.at[n], out.at[i, h], out_sems.at[n]))
        backs[-1].start()
    for c in extra + backs:
        c.wait()


def output_kernel(hidden, w_out, own, other, *, seqs):
    total = product(hidden[...], w_out[...])
    term = total.astype(BF16)
    half, share = own.shape[0], seqs // 2
    me = lax.axis_index("tp")
    r = lax.broadcasted_iota(jnp.int32, (half, 2 * half), 0)
    c = lax.broadcasted_iota(jnp.int32, (half, 2 * half), 1)
    at = (r // share) * seqs + r % share
    own[...] = product((c == at + me * share).astype(BF16), term).astype(BF16)
    other[...] = product((c == at + (1 - me) * share).astype(BF16), term).astype(BF16)


def resid_kernel(raw, mixed, gain, ffn, mine, resid):
    members, rows, cols = mixed.shape
    group = max(1, 128 // cols)
    total = None
    for n in range(0, members, group):
        part = jnp.concatenate([mixed[n + g] for g in range(group)], axis=1) if group > 1 else mixed[n]
        at = slice(n * cols, (n + group) * cols)
        block = raw[:, at].astype(F32) + part.astype(F32)
        resid[:, at] = block
        squares = jnp.sum(block * block, axis=1, keepdims=True)
        total = squares if total is None else total + squares
    scale = lax.rsqrt(total / (members * cols) + 1e-06)
    ffn[...] = (resid[...] * scale * gain[...]).astype(BF16)
    share = mine.shape[0]
    me = lax.axis_index("ep")
    for j in range(share):
        mine[j : j + 1] = resid[pl.ds(me * share + j, 1)]


def join_kernel(own, other, out):
    share = out.shape[1]
    both = own[...].astype(F32) + other[...].astype(F32)
    for e in range(out.shape[0]):
        out[e] = both[e * share : (e + 1) * share].astype(BF16)


def share_kernel(tokens, out):
    share = out.shape[1]
    me = lax.axis_index("tp")
    values = tokens[...].astype(F32)
    mine = jnp.where(me == 0, values[0:share], values[share:]).astype(BF16)
    for e in range(out.shape[0]):
        out[e] = mine


def gates_kernel(tokens, gain, w_in, w_forget, bias, stab, stab_out, decay, inweight, floor):
    normed = rms_scale(tokens[...].astype(F32), gain[...]).astype(BF16)
    in_pre = product_t(normed, w_in[...])
    old = jax.nn.log_sigmoid(product_t(normed, w_forget[...]) + bias[...]) + stab[...]
    new = jnp.maximum(old, in_pre)
    stab_out[...] = new
    decay[...] = jnp.exp(old - new)
    inweight[...] = jnp.exp(in_pre - new)
    floor[...] = jnp.exp(-new)


def body(
    tokens,
    memory,
    normalizer,
    stabilizer,
    norm_gain,
    w_query,
    w_key,
    w_value,
    w_outgate,
    w_input,
    w_forget,
    forget_bias,
    w_out,
    ffn_gain,
    w_gate,
    w_up,
    w_down,
    expert_ids,
    route_weights,
):
    n_ep = lax.axis_size("ep")
    n_tp = lax.axis_size("tp")
    assert n_tp == 2
    me_tp = lax.axis_index("tp")
    swap = [(0, 1), (1, 0)]
    seqs, width = tokens.shape
    share = seqs // n_tp
    half = n_ep * share
    heads, key_size, value_size = (memory.shape[1], memory.shape[2], memory.shape[3])
    value_width = heads * value_size
    key_piece = w_query.shape[2]
    value_piece = w_value.shape[2]
    narrow = heads * key_piece
    broad = heads * value_piece
    total = 2 * narrow + 2 * broad

    copies = call(share_kernel, shape((n_ep, share, width), BF16), [VMEM], [], [tokens], "share")
    raw_own = to_all(copies).reshape(half, width)
    raw_other = lax.ppermute(raw_own, "tp", swap)

    columns = [jnp.transpose(w, (1, 2, 0)).reshape(-1, width) for w in (w_query, w_key, w_value, w_outgate)]
    cut = 2 * narrow + broad
    gain, front, normed_own = call(
        front_kernel,
        (pltpu.VMEM((1, width), F32), pltpu.VMEM((cut, width), BF16), shape((half, width), BF16)),
        [VMEM] + [HBM] * 4,
        [pltpu.SemaphoreType.DMA((4,))],
        [raw_own, norm_gain.reshape(1, width), *columns[:3]],
        "front",
        flops=10**7,
    )
    projected = call(
        functools.partial(project_kernel, seqs=seqs),
        shape((n_ep, seqs, total), BF16),
        [VMEM, VMEM, FAST, FAST, HBM],
        [pltpu.VMEM((broad, width), BF16), pltpu.VMEM((2 * half, width), BF16), pltpu.SemaphoreType.DMA((1,))],
        [normed_own, raw_other, gain, front, columns[3]],
        "project",
        flops=2 * 2 * half * total * width,
    )
    n_cells = seqs * heads
    near = n_cells * 3 // 8
    first = call(
        recall_kernel,
        pltpu.VMEM((near, key_size, value_size), F32),
        [ANY, HBM],
        [pltpu.SemaphoreType.DMA((near,))],
        [projected, memory],
        "recall",
        flops=10**7,
    )
    pieces = to_all(projected)

    stab_next, decay, inweight, floor = call(
        gates_kernel,
        (shape((seqs, heads), F32),) * 4,
        [VMEM] * 6,
        [],
        [tokens, norm_gain.reshape(1, width), w_input.T, w_forget.T, forget_bias.reshape(1, heads), stabilizer],
        "gates",
    )

    hidden, norm_next, key, value = call(
        functools.partial(readout_kernel, piece=(key_piece, value_piece)),
        (
            pltpu.HBM((n_ep, seqs, value_width), BF16),
            shape(normalizer.shape, F32),
            shape((heads * 8, key_size), F32),
            shape((seqs, value_width), F32),
        ),
        [VMEM] * 5 + [FAST, HBM],
        [
            pltpu.VMEM((n_cells - near, key_size, value_size), F32),
            pltpu.VMEM((seqs, value_width), F32),
            pltpu.VMEM((seqs, value_width), BF16),
            pltpu.SemaphoreType.DMA((n_cells - near,)),
            pltpu.SemaphoreType.DMA((n_ep,)),
        ],
        [pieces, decay, inweight, floor, normalizer, first, memory],
        "readout",
        flops=2 * memory.size,
        outs=(HBM, VMEM, VMEM, VMEM),
    )
    hidden_all = to_all(hidden).reshape(n_ep * seqs, value_width)
    memory_next, w_out_near = call(
        update_kernel,
        (shape(memory.shape, F32), pltpu.VMEM(w_out.shape, BF16)),
        [VMEM] * 4 + [HBM] * 2,
        [
            pltpu.VMEM((n_cells, key_size, value_size), F32),
            pltpu.SemaphoreType.DMA((n_cells,)),
            pltpu.SemaphoreType.DMA((n_cells,)),
            pltpu.SemaphoreType.DMA((1,)),
        ],
        [key, value, decay, inweight, w_out, memory],
        "update",
        flops=10**8,
        outs=(HBM, VMEM),
    )

    own_term, other_term = call(
        functools.partial(output_kernel, seqs=seqs),
        (shape((half, w_out.shape[1]), BF16),) * 2,
        [VMEM, FAST],
        [],
        [hidden_all, w_out_near],
        "output",
        flops=2 * n_ep * seqs * w_out.size,
    )
    mixed = (own_term.astype(F32) + lax.ppermute(other_term, "tp", swap).astype(F32)).astype(BF16)
    mixed_all = to_all(jnp.broadcast_to(mixed[None], (n_ep,) + mixed.shape))

    ffn_own, resid_mine = call(
        resid_kernel,
        (shape((half, width), BF16), shape((share, width), F32)),
        [VMEM] * 3,
        [pltpu.VMEM((half, width), F32)],
        [raw_own, mixed_all, ffn_gain.reshape(1, width)],
        "resid",
    )
    ffn_other = lax.ppermute(ffn_own, "tp", swap)
    units = w_gate.shape[2]
    units_near = call(
        units_kernel,
        pltpu.VMEM((width // 2, 2 * units), BF16),
        [ANY, HBM, HBM],
        [pltpu.SemaphoreType.DMA((4,))],
        [ffn_own, w_gate, w_up],
        "units",
        flops=10**7,
    )
    act_own, down, down_other = call(
        expert_kernel,
        (shape((half, units), BF16), pltpu.VMEM((units, width), BF16), shape((half, width), BF16)),
        [VMEM, VMEM, FAST, HBM, HBM, HBM],
        [
            pltpu.VMEM((width // 2, 2 * units), BF16),
            pltpu.SemaphoreType.DMA((4,)),
            pltpu.SemaphoreType.DMA((4,)),
        ],
        [ffn_own, ffn_other, units_near, w_gate, w_up, w_down],
        "experts",
        flops=2 * 3 * half * width * units,
    )
    down_own = call(
        down_kernel, shape((half, width), BF16), [VMEM, FAST], [], [act_own, down], "down", flops=10**7
    )
    summed = call(
        join_kernel,
        shape((n_ep, share, width), BF16),
        [VMEM] * 2,
        [],
        [down_own, lax.ppermute(down_other, "tp", swap)],
        "join",
    )
    by_expert = to_all(summed)

    n_experts = n_ep * w_gate.shape[0]
    labels = jnp.arange(n_experts, dtype=jnp.int32)
    ids = lax.dynamic_slice_in_dim(expert_ids, me_tp * share, share, 0)
    gains = lax.dynamic_slice_in_dim(route_weights, me_tp * share, share, 0)
    route = jnp.sum(jnp.where(ids[:, :, None] == labels[None, None, :], gains[:, :, None], 0.0), axis=1)
    ffn_out = jnp.sum(by_expert.astype(F32) * jnp.swapaxes(route, 0, 1)[:, :, None], axis=0)
    out_mine = (resid_mine + ffn_out).astype(BF16)
    out_other = lax.ppermute(out_mine, "tp", swap)
    first = jnp.where(me_tp == 0, out_mine, out_other)
    last = jnp.where(me_tp == 0, out_other, out_mine)
    out = jnp.concatenate([first, last], axis=0)
    return (out, memory_next, norm_next, stab_next)


def solution(mesh):
    return jax.shard_map(
        body,
        mesh=mesh,
        in_specs=(
            P("ep", None),
            P("ep", "tp", None, None),
            P("ep", "tp", None),
            P("ep", "tp"),
            P(),
            P(None, "tp", "ep"),
            P(None, "tp", "ep"),
            P(None, "tp", "ep"),
            P(None, "tp", "ep"),
            P(None, "tp"),
            P(None, "tp"),
            P("tp"),
            P("tp", "ep"),
            P(),
            P("ep", None, "tp"),
            P("ep", None, "tp"),
            P("ep", "tp", None),
            P("ep", None),
            P("ep", None),
        ),
        out_specs=(P("ep", None), P("ep", "tp", None, None), P("ep", "tp", None), P("ep", "tp")),
        check_vma=False,
    )
```

```python
import functools

import jax
import jax.numpy as jnp
from jax import lax
from jax.experimental import pallas as pl
from jax.experimental.pallas import tpu as pltpu
from jax.sharding import PartitionSpec as P

F32 = jnp.float32
LONG = 10**11
BF16 = jnp.bfloat16
ANY = pl.BlockSpec(memory_space=pl.ANY)
HBM = pl.BlockSpec(memory_space=pltpu.HBM)
VMEM = pl.BlockSpec(memory_space=pltpu.VMEM)
FAST = pl.BlockSpec(memory_space=pltpu.VMEM)


def rms_scale(values, gain):
    return values * lax.rsqrt(jnp.mean(values * values, axis=-1, keepdims=True) + 1e-06) * gain


def product(left, right):
    return jnp.dot(left, right, preferred_element_type=F32)


def product_t(left, right):
    return lax.dot_general(left, right, (((1,), (1,)), ((), ())), preferred_element_type=F32)


def to_all(copies):
    return lax.all_to_all(copies, "ep", split_axis=0, concat_axis=0, tiled=True)


def call(kernel, out_shape, in_specs, scratch, args, name, flops=10**6, outs=None, nbytes=10**6):
    many = isinstance(out_shape, tuple)
    outs = outs or (tuple(VMEM for _ in out_shape) if many else VMEM)
    pins = {id(HBM): pltpu.HBM, id(FAST): pltpu.VMEM}
    args = [pltpu.with_memory_space_constraint(a, pins[id(s)]) if id(s) in pins else a for a, s in zip(args, in_specs)]
    return pl.pallas_call(
        kernel,
        out_shape=out_shape,
        in_specs=in_specs,
        out_specs=outs,
        scratch_shapes=scratch,
        name=name,
        compiler_params=pltpu.CompilerParams(vmem_limit_bytes=24 << 20),
        cost_estimate=pl.CostEstimate(flops=flops, transcendentals=0, bytes_accessed=nbytes),
    )(*args)


def shape(dims, dtype):
    return jax.ShapeDtypeStruct(dims, dtype)


def fetch(pairs, sems):
    copies = [pltpu.make_async_copy(src, dst, sems.at[n]) for n, (src, dst) in enumerate(pairs)]
    for c in copies:
        c.start()
    return copies


def stack(blocks):
    return jnp.concatenate([blocks[e].astype(F32) for e in range(blocks.shape[0])], axis=0)


def front_kernel(own, gain, raw, normed):
    rows = stack(own)
    raw[...] = rows.astype(BF16)
    normed[...] = rms_scale(rows, gain[...]).astype(BF16)


def project_kernel(own, other, gain, wq, wk, wv, wo, after, out, normed, *, seqs):
    half = own.shape[0]
    normed[0:half] = own[...]
    normed[half:] = rms_scale(stack(other), gain[...]).astype(BF16)
    rows = 2 * half
    share = seqs // 2
    me = lax.axis_index("tp")
    r = lax.broadcasted_iota(jnp.int32, (rows, rows), 0)
    c = lax.broadcasted_iota(jnp.int32, (rows, rows), 1)
    token = r % seqs
    which = (token // share + me) % 2
    pick = (c == which * half + (r // seqs) * share + token % share).astype(BF16)
    found = [product_t(w[...], normed[...]).astype(BF16) for w in (wq, wk, wv, wo)]
    found = product_t(pick, jnp.concatenate(found, axis=0))
    for d in range(rows // seqs):
        out[d] = found[d * seqs : (d + 1) * seqs].astype(BF16)


def expert_kernel(own, other, w_gate, w_up, w_down, act_own, out):
    left = jnp.concatenate([own[...], other[...]], axis=0)
    gate = product(left, w_gate[0])
    act = (jax.nn.silu(gate) * product(left, w_up[0])).astype(BF16)
    half = own.shape[0]
    act_own[...] = act[0:half]
    out[...] = product(act[half:], w_down[0]).astype(BF16)


def down_kernel(act, w_down, out):
    out[...] = product(act[...], w_down[0]).astype(BF16)


def spread(pieces, start, piece, blocks, seqs):
    rows, total = pieces.shape
    members = rows // seqs
    low = start // 128 * 128
    high = min(total, -(-(start + blocks * piece) // 128) * 128)
    entries = members * piece
    wide = blocks * entries
    d = lax.broadcasted_iota(jnp.int32, (1, wide), 1)
    target = start - low + (d // entries) * piece + d % piece
    column = lax.broadcasted_iota(jnp.int32, (high - low, wide), 0)
    placed = product(pieces[:, low:high], jnp.where(column == target, 1.0, 0.0).astype(BF16))
    member = (d % entries) // piece
    r = lax.broadcasted_iota(jnp.int32, (rows, wide), 0) // seqs
    placed = jnp.where(r == member, placed, 0.0).astype(BF16)
    t = lax.broadcasted_iota(jnp.int32, (8, rows), 0)
    gather = jnp.where(lax.broadcasted_iota(jnp.int32, (8, rows), 1) % seqs == t, 1.0, 0.0)
    return product(gather.astype(BF16), placed)


def readout_kernel(
    pieces,
    decay,
    inweight,
    floor,
    norm,
    memory,
    out,
    norm_out,
    key_out,
    value_out,
    recalled,
    hidden,
    out_sems,
    *,
    piece,
):
    seqs, heads, dk, dv = memory.shape
    rows = jnp.concatenate([pieces[m].astype(F32) for m in range(pieces.shape[0])], axis=0).astype(BF16)
    small, large = piece
    narrow = spread(rows, 0, small, 2 * heads, seqs)
    key_at = heads * dk
    query = [narrow[:, h * dk : (h + 1) * dk] * dk ** (-0.5) for h in range(heads)]
    key = [narrow[:, key_at + h * dk : key_at + (h + 1) * dk] for h in range(heads)]
    columns = jnp.concatenate(query, axis=0).T

    def recall(cell, i, h):
        n = h * 8 + i
        part = jnp.sum(cell * columns[:, n : n + 1], axis=0, keepdims=True)
        recalled[i : i + 1, h * dv : (h + 1) * dv] = part

    for i in range(seqs):
        for h in range(heads):
            recall(memory[i, h], i, h)
    value = spread(rows, 2 * heads * small, large, heads, seqs)[0:seqs]
    outgate = spread(rows, 2 * heads * small + heads * large, large, heads, seqs)[0:seqs]
    value_out[...] = value
    below, along = [], []
    for h in range(heads):
        key_out[h * 8 : (h + 1) * 8] = key[h]
        q, k = query[h][0:seqs], key[h][0:seqs]
        old = jnp.concatenate([norm[i, h : h + 1] for i in range(seqs)], axis=0)
        w = inweight[:, h : h + 1]
        new = decay[:, h : h + 1] * old + w * k
        for i in range(seqs):
            norm_out[i, h : h + 1] = new[i : i + 1]
        below.append(jnp.maximum(jnp.abs(jnp.sum(q * new, axis=1, keepdims=True)), floor[:, h : h + 1]))
        along.append(w * jnp.sum(q * k, axis=1, keepdims=True))
    gate = jax.nn.sigmoid(outgate)
    for h in range(heads):
        at = slice(h * dv, (h + 1) * dv)
        top = decay[:, h : h + 1] * recalled[:, at] + along[h] * value[:, at]
        hidden[:, at] = (top / below[h] * gate[:, at]).astype(BF16)
    for c in fetch([(hidden, out.at[e]) for e in range(out.shape[0])], out_sems):
        c.wait()


def update_kernel(key, value, decay, inweight, w_out, memory, out, w_copy, buf, sems, out_sems, w_sems):
    seqs, heads, dk, dv = memory.shape
    cells = [(i, h) for i in range(seqs) for h in range(heads)]
    copies = fetch([(memory.at[i, h], buf.at[n]) for n, (i, h) in enumerate(cells)], sems)
    extra = fetch([(w_out, w_copy)], w_sems)
    backs = []
    columns = key[...].T
    for n, (i, h) in enumerate(cells):
        copies[n].wait()
        d = decay[i : i + 1, h : h + 1]
        row = value[i : i + 1, h * dv : (h + 1) * dv] * inweight[i : i + 1, h : h + 1]
        at = h * 8 + i
        buf[n] = d * buf[n] + columns[:, at : at + 1] * row
        backs.append(pltpu.make_async_copy(buf.at[n], out.at[i, h], out_sems.at[n]))
        backs[-1].start()
    for c in extra + backs:
        c.wait()


def output_kernel(hidden, w_out, own, other, *, seqs):
    total = product(hidden[...], w_out[...])
    term = total.astype(BF16)
    half, share = own.shape[0], seqs // 2
    me = lax.axis_index("tp")
    r = lax.broadcasted_iota(jnp.int32, (half, 2 * half), 0)
    c = lax.broadcasted_iota(jnp.int32, (half, 2 * half), 1)
    at = (r // share) * seqs + r % share
    own[...] = product((c == at + me * share).astype(BF16), term).astype(BF16)
    other[...] = product((c == at + (1 - me) * share).astype(BF16), term).astype(BF16)


def resid_kernel(raw, mixed, gain, ffn, mine, resid):
    members, rows, cols = mixed.shape
    group = max(1, 128 // cols)
    total = None
    for n in range(0, members, group):
        part = jnp.concatenate([mixed[n + g] for g in range(group)], axis=1) if group > 1 else mixed[n]
        at = slice(n * cols, (n + group) * cols)
        block = raw[:, at].astype(F32) + part.astype(F32)
        resid[:, at] = block
        squares = jnp.sum(block * block, axis=1, keepdims=True)
        total = squares if total is None else total + squares
    scale = lax.rsqrt(total / (members * cols) + 1e-06)
    ffn[...] = (resid[...] * scale * gain[...]).astype(BF16)
    share = mine.shape[0]
    me = lax.axis_index("ep")
    for j in range(share):
        mine[j : j + 1] = resid[pl.ds(me * share + j, 1)]


def join_kernel(own, other, out):
    share = out.shape[1]
    both = own[...].astype(F32) + other[...].astype(F32)
    for e in range(out.shape[0]):
        out[e] = both[e * share : (e + 1) * share].astype(BF16)


def share_kernel(tokens, out):
    share = out.shape[1]
    me = lax.axis_index("tp")
    values = tokens[...].astype(F32)
    mine = jnp.where(me == 0, values[0:share], values[share:]).astype(BF16)
    for e in range(out.shape[0]):
        out[e] = mine


def gates_kernel(
    tokens, gain, w_in, w_forget, bias, stab, ids, weights, after, stab_out, decay, inweight, floor, route
):
    normed = rms_scale(tokens[...].astype(F32), gain[...]).astype(BF16)
    in_pre = product_t(normed, w_in[...])
    old = jax.nn.log_sigmoid(product_t(normed, w_forget[...]) + bias[...]) + stab[...]
    new = jnp.maximum(old, in_pre)
    stab_out[...] = new
    decay[...] = jnp.exp(old - new)
    inweight[...] = jnp.exp(in_pre - new)
    floor[...] = jnp.exp(-new)
    share, experts = route.shape
    seqs = ids.shape[1]
    label = lax.broadcasted_iota(jnp.int32, (seqs, experts), 1)
    same = lax.broadcasted_iota(jnp.int32, (seqs, seqs), 0) == lax.broadcasted_iota(jnp.int32, (seqs, seqs), 1)

    def column(row):
        return jnp.sum(jnp.where(same, row, 0.0), axis=1, keepdims=True)

    dense = jnp.zeros(label.shape, F32)
    for k in range(ids.shape[0]):
        chosen = column(ids[k : k + 1].astype(F32)).astype(jnp.int32)
        dense = dense + jnp.where(chosen == label, column(weights[k : k + 1]), 0.0)
    route[...] = jnp.where(lax.axis_index("tp") == 0, dense[0:share], dense[share:])


def finish_kernel(terms, route, resid, out):
    total = resid[...]
    for e in range(terms.shape[0]):
        total = total + route[:, e : e + 1] * terms[e].astype(F32)
    out[...] = total.astype(BF16)


def merge_kernel(mine, other, out):
    share = mine.shape[0]
    first = lax.axis_index("tp") == 0
    a, b = mine[...].astype(F32), other[...].astype(F32)
    out[0:share] = jnp.where(first, a, b).astype(BF16)
    out[share:] = jnp.where(first, b, a).astype(BF16)


def body(
    tokens,
    memory,
    normalizer,
    stabilizer,
    norm_gain,
    w_query,
    w_key,
    w_value,
    w_outgate,
    w_input,
    w_forget,
    forget_bias,
    w_out,
    ffn_gain,
    w_gate,
    w_up,
    w_down,
    expert_ids,
    route_weights,
):
    n_ep = lax.axis_size("ep")
    n_tp = lax.axis_size("tp")
    assert n_tp == 2
    swap = [(0, 1), (1, 0)]
    seqs, width = tokens.shape
    share = seqs // n_tp
    half = n_ep * share
    heads, key_size, value_size = (memory.shape[1], memory.shape[2], memory.shape[3])
    value_width = heads * value_size
    key_piece = w_query.shape[2]
    value_piece = w_value.shape[2]
    narrow = heads * key_piece
    broad = heads * value_piece
    total = 2 * narrow + 2 * broad

    copies = call(share_kernel, shape((n_ep, share, width), BF16), [VMEM], [], [tokens], "share", flops=LONG)
    gathered = to_all(copies)
    gathered_other = lax.ppermute(gathered, "tp", swap)
    raw_own, normed_own = call(
        front_kernel,
        (shape((half, width), BF16),) * 2,
        [VMEM] * 2,
        [],
        [gathered, norm_gain.reshape(1, width)],
        "front",
    )
    n_experts = n_ep * w_gate.shape[0]
    stab_next, decay, inweight, floor, route = call(
        gates_kernel,
        (shape((seqs, heads), F32),) * 4 + (shape((share, n_experts), F32),),
        [VMEM] * 8 + [ANY],
        [],
        [
            tokens,
            norm_gain.reshape(1, width),
            w_input.T,
            w_forget.T,
            forget_bias.reshape(1, heads),
            stabilizer,
            expert_ids.T,
            route_weights.T,
            normed_own,
        ],
        "gates",
    )
    columns = [jnp.transpose(w, (1, 2, 0)).reshape(-1, width) for w in (w_query, w_key, w_value, w_outgate)]
    projected = call(
        functools.partial(project_kernel, seqs=seqs),
        shape((n_ep, seqs, total), BF16),
        [VMEM] * 7 + [ANY],
        [pltpu.VMEM((2 * half, width), BF16)],
        [normed_own, gathered_other, norm_gain.reshape(1, width), *columns, route],
        "project",
        flops=LONG,
    )
    n_cells = seqs * heads
    pieces = to_all(projected)

    hidden, norm_next, key, value = call(
        functools.partial(readout_kernel, piece=(key_piece, value_piece)),
        (
            pltpu.HBM((n_ep, seqs, value_width), BF16),
            shape(normalizer.shape, F32),
            shape((heads * 8, key_size), F32),
            shape((seqs, value_width), F32),
        ),
        [VMEM] * 6,
        [
            pltpu.VMEM((seqs, value_width), F32),
            pltpu.VMEM((seqs, value_width), BF16),
            pltpu.SemaphoreType.DMA((n_ep,)),
        ],
        [pieces, decay, inweight, floor, normalizer, memory],
        "readout",
        flops=2 * memory.size,
        outs=(HBM, VMEM, VMEM, VMEM),
    )
    hidden_all = to_all(hidden).reshape(n_ep * seqs, value_width)
    memory_next, w_out_near = call(
        update_kernel,
        (shape(memory.shape, F32), pltpu.VMEM(w_out.shape, BF16)),
        [VMEM] * 4 + [HBM] * 2,
        [
            pltpu.VMEM((n_cells, key_size, value_size), F32),
            pltpu.SemaphoreType.DMA((n_cells,)),
            pltpu.SemaphoreType.DMA((n_cells,)),
            pltpu.SemaphoreType.DMA((1,)),
        ],
        [key, value, decay, inweight, w_out, memory],
        "update",
        flops=10**8,
        outs=(HBM, VMEM),
    )

    own_term, other_term = call(
        functools.partial(output_kernel, seqs=seqs),
        (shape((half, w_out.shape[1]), BF16),) * 2,
        [VMEM, FAST],
        [],
        [hidden_all, w_out_near],
        "output",
        flops=LONG,
    )
    mixed = (own_term.astype(F32) + lax.ppermute(other_term, "tp", swap).astype(F32)).astype(BF16)
    mixed_all = to_all(jnp.broadcast_to(mixed[None], (n_ep,) + mixed.shape))

    ffn_own, resid_mine = call(
        resid_kernel,
        (shape((half, width), BF16), shape((share, width), F32)),
        [VMEM] * 3,
        [pltpu.VMEM((half, width), F32)],
        [raw_own, mixed_all, ffn_gain.reshape(1, width)],
        "resid",
    )
    ffn_other = lax.ppermute(ffn_own, "tp", swap)
    units = w_gate.shape[2]
    act_own, down_other = call(
        expert_kernel,
        (shape((half, units), BF16), shape((half, width), BF16)),
        [VMEM] * 5,
        [],
        [ffn_own, ffn_other, w_gate, w_up, w_down],
        "experts",
        flops=2 * 3 * half * width * units,
    )
    down_own = call(
        down_kernel, shape((half, width), BF16), [VMEM] * 2, [], [act_own, w_down], "down", flops=10**7
    )
    summed = call(
        join_kernel,
        shape((n_ep, share, width), BF16),
        [VMEM] * 2,
        [],
        [down_own, lax.ppermute(down_other, "tp", swap)],
        "join",
    )
    by_expert = to_all(summed)

    out_mine = call(
        finish_kernel, shape((share, width), BF16), [VMEM] * 3, [], [by_expert, route, resid_mine], "finish"
    )
    out = call(
        merge_kernel,
        shape((seqs, width), BF16),
        [VMEM] * 2,
        [],
        [out_mine, lax.ppermute(out_mine, "tp", swap)],
        "merge",
    )
    return (out, memory_next, norm_next, stab_next)


def solution(mesh):
    return jax.shard_map(
        body,
        mesh=mesh,
        in_specs=(
            P("ep", None),
            P("ep", "tp", None, None),
            P("ep", "tp", None),
            P("ep", "tp"),
            P(),
            P(None, "tp", "ep"),
            P(None, "tp", "ep"),
            P(None, "tp", "ep"),
            P(None, "tp", "ep"),
            P(None, "tp"),
            P(None, "tp"),
            P("tp"),
            P("tp", "ep"),
            P(),
            P("ep", None, "tp"),
            P("ep", None, "tp"),
            P("ep", "tp", None),
            P("ep", None),
            P("ep", None),
        ),
        out_specs=(P("ep", None), P("ep", "tp", None, None), P("ep", "tp", None), P("ep", "tp")),
        check_vma=False,
    )
```

```python
import functools

import jax
import jax.numpy as jnp
from jax import lax
from jax.experimental import pallas as pl
from jax.experimental.pallas import tpu as pltpu
from jax.sharding import PartitionSpec as P

F32 = jnp.float32
LONG = 10**11
BF16 = jnp.bfloat16
ANY = pl.BlockSpec(memory_space=pl.ANY)
HBM = pl.BlockSpec(memory_space=pltpu.HBM)
VMEM = pl.BlockSpec(memory_space=pltpu.VMEM)
FAST = pl.BlockSpec(memory_space=pltpu.VMEM)


def rms_scale(values, gain):
    return values * lax.rsqrt(jnp.mean(values * values, axis=-1, keepdims=True) + 1e-06) * gain


def product(left, right):
    return jnp.dot(left, right, preferred_element_type=F32)


def product_t(left, right):
    return lax.dot_general(left, right, (((1,), (1,)), ((), ())), preferred_element_type=F32)


def to_all(copies):
    return lax.all_to_all(copies, "ep", split_axis=0, concat_axis=0, tiled=True)


def call(kernel, out_shape, in_specs, scratch, args, name, flops=10**6, outs=None, nbytes=10**6):
    many = isinstance(out_shape, tuple)
    outs = outs or (tuple(VMEM for _ in out_shape) if many else VMEM)
    pins = {id(HBM): pltpu.HBM, id(FAST): pltpu.VMEM}
    args = [pltpu.with_memory_space_constraint(a, pins[id(s)]) if id(s) in pins else a for a, s in zip(args, in_specs)]
    return pl.pallas_call(
        kernel,
        out_shape=out_shape,
        in_specs=in_specs,
        out_specs=outs,
        scratch_shapes=scratch,
        name=name,
        compiler_params=pltpu.CompilerParams(vmem_limit_bytes=24 << 20),
        cost_estimate=pl.CostEstimate(flops=flops, transcendentals=0, bytes_accessed=nbytes),
    )(*args)


def shape(dims, dtype):
    return jax.ShapeDtypeStruct(dims, dtype)


def fetch(pairs, sems):
    copies = [pltpu.make_async_copy(src, dst, sems.at[n]) for n, (src, dst) in enumerate(pairs)]
    for c in copies:
        c.start()
    return copies


def stack(blocks):
    return jnp.concatenate([blocks[e].astype(F32) for e in range(blocks.shape[0])], axis=0)


def front_kernel(own, gain, raw, normed):
    rows = stack(own)
    raw[...] = rows.astype(BF16)
    normed[...] = rms_scale(rows, gain[...]).astype(BF16)


def project_kernel(own, other, gain, wq, wk, wv, wo, after, out, normed, *, seqs):
    half = own.shape[0]
    normed[0:half] = own[...]
    normed[half:] = rms_scale(stack(other), gain[...]).astype(BF16)
    rows = 2 * half
    share = seqs // 2
    me = lax.axis_index("tp")
    r = lax.broadcasted_iota(jnp.int32, (rows, rows), 0)
    c = lax.broadcasted_iota(jnp.int32, (rows, rows), 1)
    token = r % seqs
    which = (token // share + me) % 2
    pick = (c == which * half + (r // seqs) * share + token % share).astype(BF16)
    found = [product_t(w[...], normed[...]).astype(BF16) for w in (wq, wk, wv, wo)]
    found = product_t(pick, jnp.concatenate(found, axis=0))
    for d in range(rows // seqs):
        out[d] = found[d * seqs : (d + 1) * seqs].astype(BF16)


def expert_kernel(own, other, w_gate, w_up, w_down, act_own, out):
    left = jnp.concatenate([own[...], other[...]], axis=0)
    gate = product(left, w_gate[0])
    act = (jax.nn.silu(gate) * product(left, w_up[0])).astype(BF16)
    half = own.shape[0]
    act_own[...] = act[0:half]
    out[...] = product(act[half:], w_down[0]).astype(BF16)


def down_kernel(act, w_down, out):
    out[...] = product(act[...], w_down[0]).astype(BF16)


def spread(pieces, start, piece, blocks, seqs):
    rows, total = pieces.shape
    members = rows // seqs
    low = start // 128 * 128
    high = min(total, -(-(start + blocks * piece) // 128) * 128)
    entries = members * piece
    wide = blocks * entries
    d = lax.broadcasted_iota(jnp.int32, (1, wide), 1)
    target = start - low + (d // entries) * piece + d % piece
    column = lax.broadcasted_iota(jnp.int32, (high - low, wide), 0)
    placed = product(pieces[:, low:high], jnp.where(column == target, 1.0, 0.0).astype(BF16))
    member = (d % entries) // piece
    r = lax.broadcasted_iota(jnp.int32, (rows, wide), 0) // seqs
    placed = jnp.where(r == member, placed, 0.0).astype(BF16)
    t = lax.broadcasted_iota(jnp.int32, (8, rows), 0)
    gather = jnp.where(lax.broadcasted_iota(jnp.int32, (8, rows), 1) % seqs == t, 1.0, 0.0)
    return product(gather.astype(BF16), placed)


def readout_kernel(
    pieces,
    decay,
    inweight,
    floor,
    norm,
    memory,
    out,
    norm_out,
    key_out,
    value_out,
    recalled,
    hidden,
    norm_new,
    out_sems,
    norm_sems,
    *,
    piece,
):
    seqs, heads, dk, dv = memory.shape
    rows = jnp.concatenate([pieces[m].astype(F32) for m in range(pieces.shape[0])], axis=0).astype(BF16)
    small, large = piece
    narrow = spread(rows, 0, small, 2 * heads, seqs)
    key_at = heads * dk
    query = [narrow[:, h * dk : (h + 1) * dk] * dk ** (-0.5) for h in range(heads)]
    key = [narrow[:, key_at + h * dk : key_at + (h + 1) * dk] for h in range(heads)]
    columns = jnp.concatenate(query, axis=0).T

    def recall(cell, i, h):
        n = h * 8 + i
        part = jnp.sum(cell * columns[:, n : n + 1], axis=0, keepdims=True)
        recalled[i : i + 1, h * dv : (h + 1) * dv] = part

    for i in range(seqs):
        for h in range(heads):
            recall(memory[i, h], i, h)
    value = spread(rows, 2 * heads * small, large, heads, seqs)[0:seqs]
    outgate = spread(rows, 2 * heads * small + heads * large, large, heads, seqs)[0:seqs]
    value_out[...] = value
    below, along = [], []
    for h in range(heads):
        key_out[h * 8 : (h + 1) * 8] = key[h]
        q, k = query[h][0:seqs], key[h][0:seqs]
        old = jnp.concatenate([norm[i, h : h + 1] for i in range(seqs)], axis=0)
        w = inweight[:, h : h + 1]
        new = decay[:, h : h + 1] * old + w * k
        for i in range(seqs):
            norm_new[i, h : h + 1] = new[i : i + 1]
        below.append(jnp.maximum(jnp.abs(jnp.sum(q * new, axis=1, keepdims=True)), floor[:, h : h + 1]))
        along.append(w * jnp.sum(q * k, axis=1, keepdims=True))
    backs = fetch([(norm_new, norm_out)], norm_sems)
    gate = jax.nn.sigmoid(outgate)
    for h in range(heads):
        at = slice(h * dv, (h + 1) * dv)
        top = decay[:, h : h + 1] * recalled[:, at] + along[h] * value[:, at]
        hidden[:, at] = (top / below[h] * gate[:, at]).astype(BF16)
    for c in fetch([(hidden, out.at[e]) for e in range(out.shape[0])], out_sems) + backs:
        c.wait()


def update_kernel(key, value, decay, inweight, w_out, memory, out, w_copy, buf, sems, out_sems, w_sems):
    seqs, heads, dk, dv = memory.shape
    cells = [(i, h) for i in range(seqs) for h in range(heads)]
    copies = fetch([(memory.at[i, h], buf.at[n]) for n, (i, h) in enumerate(cells)], sems)
    extra = fetch([(w_out, w_copy)], w_sems)
    backs = []
    columns = key[...].T
    for n, (i, h) in enumerate(cells):
        copies[n].wait()
        d = decay[i : i + 1, h : h + 1]
        row = value[i : i + 1, h * dv : (h + 1) * dv] * inweight[i : i + 1, h : h + 1]
        at = h * 8 + i
        buf[n] = d * buf[n] + columns[:, at : at + 1] * row
        backs.append(pltpu.make_async_copy(buf.at[n], out.at[i, h], out_sems.at[n]))
        backs[-1].start()
    for c in extra + backs:
        c.wait()


def output_kernel(hidden, w_out, own, other, *, seqs):
    total = product(hidden[...], w_out[...])
    term = total.astype(BF16)
    half, share = own.shape[0], seqs // 2
    me = lax.axis_index("tp")
    r = lax.broadcasted_iota(jnp.int32, (half, 2 * half), 0)
    c = lax.broadcasted_iota(jnp.int32, (half, 2 * half), 1)
    at = (r // share) * seqs + r % share
    own[...] = product((c == at + me * share).astype(BF16), term).astype(BF16)
    other[...] = product((c == at + (1 - me) * share).astype(BF16), term).astype(BF16)


def resid_kernel(raw, mixed, gain, ffn, mine, resid):
    members, rows, cols = mixed.shape
    group = max(1, 128 // cols)
    total = None
    for n in range(0, members, group):
        part = jnp.concatenate([mixed[n + g] for g in range(group)], axis=1) if group > 1 else mixed[n]
        at = slice(n * cols, (n + group) * cols)
        block = raw[:, at].astype(F32) + part.astype(F32)
        resid[:, at] = block
        squares = jnp.sum(block * block, axis=1, keepdims=True)
        total = squares if total is None else total + squares
    scale = lax.rsqrt(total / (members * cols) + 1e-06)
    ffn[...] = (resid[...] * scale * gain[...]).astype(BF16)
    share = mine.shape[0]
    me = lax.axis_index("ep")
    for j in range(share):
        mine[j : j + 1] = resid[pl.ds(me * share + j, 1)]


def join_kernel(own, other, out):
    share = out.shape[1]
    both = own[...].astype(F32) + other[...].astype(F32)
    for e in range(out.shape[0]):
        out[e] = both[e * share : (e + 1) * share].astype(BF16)


def share_kernel(tokens, out):
    share = out.shape[1]
    me = lax.axis_index("tp")
    values = tokens[...].astype(F32)
    mine = jnp.where(me == 0, values[0:share], values[share:]).astype(BF16)
    for e in range(out.shape[0]):
        out[e] = mine


def gates_kernel(
    tokens, gain, w_in, w_forget, bias, stab, ids, weights, after, stab_out, decay, inweight, floor, route
):
    normed = rms_scale(tokens[...].astype(F32), gain[...]).astype(BF16)
    in_pre = product_t(normed, w_in[...])
    old = jax.nn.log_sigmoid(product_t(normed, w_forget[...]) + bias[...]) + stab[...]
    new = jnp.maximum(old, in_pre)
    stab_out[...] = new
    decay[...] = jnp.exp(old - new)
    inweight[...] = jnp.exp(in_pre - new)
    floor[...] = jnp.exp(-new)
    share, experts = route.shape
    seqs = ids.shape[1]
    label = lax.broadcasted_iota(jnp.int32, (seqs, experts), 1)
    same = lax.broadcasted_iota(jnp.int32, (seqs, seqs), 0) == lax.broadcasted_iota(jnp.int32, (seqs, seqs), 1)

    def column(row):
        return jnp.sum(jnp.where(same, row, 0.0), axis=1, keepdims=True)

    dense = jnp.zeros(label.shape, F32)
    for k in range(ids.shape[0]):
        chosen = column(ids[k : k + 1].astype(F32)).astype(jnp.int32)
        dense = dense + jnp.where(chosen == label, column(weights[k : k + 1]), 0.0)
    route[...] = jnp.where(lax.axis_index("tp") == 0, dense[0:share], dense[share:])


def finish_kernel(terms, route, resid, out):
    total = resid[...]
    for e in range(terms.shape[0]):
        total = total + route[:, e : e + 1] * terms[e].astype(F32)
    out[...] = total.astype(BF16)


def merge_kernel(mine, other, out):
    share = mine.shape[0]
    first = lax.axis_index("tp") == 0
    a, b = mine[...].astype(F32), other[...].astype(F32)
    out[0:share] = jnp.where(first, a, b).astype(BF16)
    out[share:] = jnp.where(first, b, a).astype(BF16)


def body(
    tokens,
    memory,
    normalizer,
    stabilizer,
    norm_gain,
    w_query,
    w_key,
    w_value,
    w_outgate,
    w_input,
    w_forget,
    forget_bias,
    w_out,
    ffn_gain,
    w_gate,
    w_up,
    w_down,
    expert_ids,
    route_weights,
):
    n_ep = lax.axis_size("ep")
    n_tp = lax.axis_size("tp")
    assert n_tp == 2
    swap = [(0, 1), (1, 0)]
    seqs, width = tokens.shape
    share = seqs // n_tp
    half = n_ep * share
    heads, key_size, value_size = (memory.shape[1], memory.shape[2], memory.shape[3])
    value_width = heads * value_size
    key_piece = w_query.shape[2]
    value_piece = w_value.shape[2]
    narrow = heads * key_piece
    broad = heads * value_piece
    total = 2 * narrow + 2 * broad

    copies = call(share_kernel, shape((n_ep, share, width), BF16), [VMEM], [], [tokens], "share", flops=LONG)
    gathered = to_all(copies)
    gathered_other = lax.ppermute(gathered, "tp", swap)
    raw_own, normed_own = call(
        front_kernel,
        (shape((half, width), BF16),) * 2,
        [VMEM] * 2,
        [],
        [gathered, norm_gain.reshape(1, width)],
        "front",
    )
    n_experts = n_ep * w_gate.shape[0]
    stab_next, decay, inweight, floor, route = call(
        gates_kernel,
        (shape((seqs, heads), F32),) * 4 + (shape((share, n_experts), F32),),
        [VMEM] * 8 + [ANY],
        [],
        [
            tokens,
            norm_gain.reshape(1, width),
            w_input.T,
            w_forget.T,
            forget_bias.reshape(1, heads),
            stabilizer,
            expert_ids.T,
            route_weights.T,
            normed_own,
        ],
        "gates",
    )
    columns = [jnp.transpose(w, (1, 2, 0)).reshape(-1, width) for w in (w_query, w_key, w_value, w_outgate)]
    projected = call(
        functools.partial(project_kernel, seqs=seqs),
        shape((n_ep, seqs, total), BF16),
        [VMEM] * 7 + [ANY],
        [pltpu.VMEM((2 * half, width), BF16)],
        [normed_own, gathered_other, norm_gain.reshape(1, width), *columns, route],
        "project",
        flops=LONG,
    )
    n_cells = seqs * heads
    pieces = to_all(projected)

    hidden, norm_next, key, value = call(
        functools.partial(readout_kernel, piece=(key_piece, value_piece)),
        (
            pltpu.HBM((n_ep, seqs, value_width), BF16),
            pltpu.HBM(normalizer.shape, F32),
            shape((heads * 8, key_size), F32),
            shape((seqs, value_width), F32),
        ),
        [VMEM] * 6,
        [
            pltpu.VMEM((seqs, value_width), F32),
            pltpu.VMEM((seqs, value_width), BF16),
            pltpu.VMEM(normalizer.shape, F32),
            pltpu.SemaphoreType.DMA((n_ep,)),
            pltpu.SemaphoreType.DMA((1,)),
        ],
        [pieces, decay, inweight, floor, normalizer, memory],
        "readout",
        flops=2 * memory.size,
        outs=(HBM, HBM, VMEM, VMEM),
    )
    hidden_all = to_all(hidden).reshape(n_ep * seqs, value_width)
    memory_next, w_out_near = call(
        update_kernel,
        (shape(memory.shape, F32), pltpu.VMEM(w_out.shape, BF16)),
        [VMEM] * 4 + [HBM] * 2,
        [
            pltpu.VMEM((n_cells, key_size, value_size), F32),
            pltpu.SemaphoreType.DMA((n_cells,)),
            pltpu.SemaphoreType.DMA((n_cells,)),
            pltpu.SemaphoreType.DMA((1,)),
        ],
        [key, value, decay, inweight, w_out, memory],
        "update",
        flops=10**8,
        outs=(HBM, VMEM),
    )

    own_term, other_term = call(
        functools.partial(output_kernel, seqs=seqs),
        (shape((half, w_out.shape[1]), BF16),) * 2,
        [VMEM, FAST],
        [],
        [hidden_all, w_out_near],
        "output",
        flops=LONG,
    )
    mixed = (own_term.astype(F32) + lax.ppermute(other_term, "tp", swap).astype(F32)).astype(BF16)
    mixed_all = to_all(jnp.broadcast_to(mixed[None], (n_ep,) + mixed.shape))

    ffn_own, resid_mine = call(
        resid_kernel,
        (shape((half, width), BF16), shape((share, width), F32)),
        [VMEM] * 3,
        [pltpu.VMEM((half, width), F32)],
        [raw_own, mixed_all, ffn_gain.reshape(1, width)],
        "resid",
    )
    ffn_other = lax.ppermute(ffn_own, "tp", swap)
    units = w_gate.shape[2]
    act_own, down_other = call(
        expert_kernel,
        (shape((half, units), BF16), shape((half, width), BF16)),
        [VMEM] * 5,
        [],
        [ffn_own, ffn_other, w_gate, w_up, w_down],
        "experts",
        flops=2 * 3 * half * width * units,
    )
    down_own = call(
        down_kernel, shape((half, width), BF16), [VMEM] * 2, [], [act_own, w_down], "down", flops=10**7
    )
    summed = call(
        join_kernel,
        shape((n_ep, share, width), BF16),
        [VMEM] * 2,
        [],
        [down_own, lax.ppermute(down_other, "tp", swap)],
        "join",
    )
    by_expert = to_all(summed)

    out_mine = call(
        finish_kernel, shape((share, width), BF16), [VMEM] * 3, [], [by_expert, route, resid_mine], "finish"
    )
    out = call(
        merge_kernel,
        shape((seqs, width), BF16),
        [VMEM] * 2,
        [],
        [out_mine, lax.ppermute(out_mine, "tp", swap)],
        "merge",
    )
    return (out, memory_next, norm_next, stab_next)


def solution(mesh):
    return jax.shard_map(
        body,
        mesh=mesh,
        in_specs=(
            P("ep", None),
            P("ep", "tp", None, None),
            P("ep", "tp", None),
            P("ep", "tp"),
            P(),
            P(None, "tp", "ep"),
            P(None, "tp", "ep"),
            P(None, "tp", "ep"),
            P(None, "tp", "ep"),
            P(None, "tp"),
            P(None, "tp"),
            P("tp"),
            P("tp", "ep"),
            P(),
            P("ep", None, "tp"),
            P("ep", None, "tp"),
            P("ep", "tp", None),
            P("ep", None),
            P("ep", None),
        ),
        out_specs=(P("ep", None), P("ep", "tp", None, None), P("ep", "tp", None), P("ep", "tp")),
        check_vma=False,
    )
```

```python
import functools

import jax
import jax.numpy as jnp
from jax import lax
from jax.experimental import pallas as pl
from jax.experimental.pallas import tpu as pltpu
from jax.sharding import PartitionSpec as P

F32 = jnp.float32
LONG = 10**11
BF16 = jnp.bfloat16
ANY = pl.BlockSpec(memory_space=pl.ANY)
HBM = pl.BlockSpec(memory_space=pltpu.HBM)
VMEM = pl.BlockSpec(memory_space=pltpu.VMEM)
FAST = pl.BlockSpec(memory_space=pltpu.VMEM)


def rms_scale(values, gain):
    return values * lax.rsqrt(jnp.mean(values * values, axis=-1, keepdims=True) + 1e-06) * gain


def product(left, right):
    return jnp.dot(left, right, preferred_element_type=F32)


def product_t(left, right):
    return lax.dot_general(left, right, (((1,), (1,)), ((), ())), preferred_element_type=F32)


def to_all(copies):
    return lax.all_to_all(copies, "ep", split_axis=0, concat_axis=0, tiled=True)


def call(kernel, out_shape, in_specs, scratch, args, name, flops=10**6, outs=None, nbytes=10**6):
    many = isinstance(out_shape, tuple)
    outs = outs or (tuple(VMEM for _ in out_shape) if many else VMEM)
    pins = {id(HBM): pltpu.HBM, id(FAST): pltpu.VMEM}
    args = [pltpu.with_memory_space_constraint(a, pins[id(s)]) if id(s) in pins else a for a, s in zip(args, in_specs)]
    return pl.pallas_call(
        kernel,
        out_shape=out_shape,
        in_specs=in_specs,
        out_specs=outs,
        scratch_shapes=scratch,
        name=name,
        compiler_params=pltpu.CompilerParams(vmem_limit_bytes=24 << 20),
        cost_estimate=pl.CostEstimate(flops=flops, transcendentals=0, bytes_accessed=nbytes),
    )(*args)


def shape(dims, dtype):
    return jax.ShapeDtypeStruct(dims, dtype)


def fetch(pairs, sems):
    copies = [pltpu.make_async_copy(src, dst, sems.at[n]) for n, (src, dst) in enumerate(pairs)]
    for c in copies:
        c.start()
    return copies


def stack(blocks):
    return jnp.concatenate([blocks[e].astype(F32) for e in range(blocks.shape[0])], axis=0)


def front_kernel(own, gain, raw, normed):
    rows = stack(own)
    raw[...] = rows.astype(BF16)
    normed[...] = rms_scale(rows, gain[...]).astype(BF16)


def project_kernel(own, other, gain, wq, wk, wv, wo, after, out, normed, *, seqs):
    half = own.shape[0]
    normed[0:half] = own[...]
    normed[half:] = rms_scale(stack(other), gain[...]).astype(BF16)
    rows = 2 * half
    share = seqs // 2
    me = lax.axis_index("tp")
    r = lax.broadcasted_iota(jnp.int32, (rows, rows), 0)
    c = lax.broadcasted_iota(jnp.int32, (rows, rows), 1)
    token = r % seqs
    which = (token // share + me) % 2
    pick = (c == which * half + (r // seqs) * share + token % share).astype(BF16)
    found = [product_t(w[...], normed[...]).astype(BF16) for w in (wq, wk, wv, wo)]
    found = product_t(pick, jnp.concatenate(found, axis=0))
    for d in range(rows // seqs):
        out[d] = found[d * seqs : (d + 1) * seqs].astype(BF16)


def expert_kernel(own, other, w_gate, w_up, w_down, act_own, out):
    left = jnp.concatenate([own[...], other[...]], axis=0)
    gate = product(left, w_gate[0])
    act = (jax.nn.silu(gate) * product(left, w_up[0])).astype(BF16)
    half = own.shape[0]
    act_own[...] = act[0:half]
    out[...] = product(act[half:], w_down[0]).astype(BF16)


def down_kernel(act, w_down, out):
    out[...] = product(act[...], w_down[0]).astype(BF16)


def spread(pieces, start, piece, blocks, seqs):
    rows, total = pieces.shape
    members = rows // seqs
    low = start // 128 * 128
    high = min(total, -(-(start + blocks * piece) // 128) * 128)
    entries = members * piece
    wide = blocks * entries
    d = lax.broadcasted_iota(jnp.int32, (1, wide), 1)
    target = start - low + (d // entries) * piece + d % piece
    column = lax.broadcasted_iota(jnp.int32, (high - low, wide), 0)
    placed = product(pieces[:, low:high], jnp.where(column == target, 1.0, 0.0).astype(BF16))
    member = (d % entries) // piece
    r = lax.broadcasted_iota(jnp.int32, (rows, wide), 0) // seqs
    placed = jnp.where(r == member, placed, 0.0).astype(BF16)
    t = lax.broadcasted_iota(jnp.int32, (8, rows), 0)
    gather = jnp.where(lax.broadcasted_iota(jnp.int32, (8, rows), 1) % seqs == t, 1.0, 0.0)
    return product(gather.astype(BF16), placed)


def readout_kernel(
    pieces,
    decay,
    inweight,
    floor,
    norm,
    memory,
    out,
    norm_out,
    key_out,
    value_out,
    recalled,
    hidden,
    norm_new,
    out_sems,
    norm_sems,
    *,
    piece,
):
    seqs, heads, dk, dv = memory.shape
    rows = jnp.concatenate([pieces[m].astype(F32) for m in range(pieces.shape[0])], axis=0).astype(BF16)
    small, large = piece
    narrow = spread(rows, 0, small, 2 * heads, seqs)
    key_at = heads * dk
    query = [narrow[:, h * dk : (h + 1) * dk] * dk ** (-0.5) for h in range(heads)]
    key = [narrow[:, key_at + h * dk : key_at + (h + 1) * dk] for h in range(heads)]
    columns = jnp.concatenate(query, axis=0).T

    def recall(cell, i, h):
        n = h * 8 + i
        part = jnp.sum(cell * columns[:, n : n + 1], axis=0, keepdims=True)
        recalled[i : i + 1, h * dv : (h + 1) * dv] = part

    value = spread(rows, 2 * heads * small, large, heads, seqs)[0:seqs]
    outgate = spread(rows, 2 * heads * small + heads * large, large, heads, seqs)[0:seqs]
    value_out[...] = value
    below, along = [], []
    for h in range(heads):
        key_out[h * 8 : (h + 1) * 8] = key[h]
        q, k = query[h][0:seqs], key[h][0:seqs]
        old = jnp.concatenate([norm[i, h : h + 1] for i in range(seqs)], axis=0)
        w = inweight[:, h : h + 1]
        new = decay[:, h : h + 1] * old + w * k
        for i in range(seqs):
            norm_new[i, h : h + 1] = new[i : i + 1]
        below.append(jnp.maximum(jnp.abs(jnp.sum(q * new, axis=1, keepdims=True)), floor[:, h : h + 1]))
        along.append(w * jnp.sum(q * k, axis=1, keepdims=True))
    backs = fetch([(norm_new, norm_out)], norm_sems)
    gate = jax.nn.sigmoid(outgate)
    for i in range(seqs):
        for h in range(heads):
            recall(memory[i, h], i, h)
    for h in range(heads):
        at = slice(h * dv, (h + 1) * dv)
        top = decay[:, h : h + 1] * recalled[:, at] + along[h] * value[:, at]
        hidden[:, at] = (top / below[h] * gate[:, at]).astype(BF16)
    for c in fetch([(hidden, out.at[e]) for e in range(out.shape[0])], out_sems) + backs:
        c.wait()


def update_kernel(key, value, decay, inweight, w_out, memory, out, w_copy, buf, sems, out_sems, w_sems):
    seqs, heads, dk, dv = memory.shape
    cells = [(i, h) for i in range(seqs) for h in range(heads)]
    copies = fetch([(memory.at[i, h], buf.at[n]) for n, (i, h) in enumerate(cells)], sems)
    extra = fetch([(w_out, w_copy)], w_sems)
    backs = []
    columns = key[...].T
    for n, (i, h) in enumerate(cells):
        copies[n].wait()
        d = decay[i : i + 1, h : h + 1]
        row = value[i : i + 1, h * dv : (h + 1) * dv] * inweight[i : i + 1, h : h + 1]
        at = h * 8 + i
        buf[n] = d * buf[n] + columns[:, at : at + 1] * row
        backs.append(pltpu.make_async_copy(buf.at[n], out.at[i, h], out_sems.at[n]))
        backs[-1].start()
    for c in extra + backs:
        c.wait()


def output_kernel(hidden, w_out, own, other, *, seqs):
    total = product(hidden[...], w_out[...])
    term = total.astype(BF16)
    half, share = own.shape[0], seqs // 2
    me = lax.axis_index("tp")
    r = lax.broadcasted_iota(jnp.int32, (half, 2 * half), 0)
    c = lax.broadcasted_iota(jnp.int32, (half, 2 * half), 1)
    at = (r // share) * seqs + r % share
    own[...] = product((c == at + me * share).astype(BF16), term).astype(BF16)
    other[...] = product((c == at + (1 - me) * share).astype(BF16), term).astype(BF16)


def resid_kernel(raw, mixed, gain, ffn, mine, resid):
    members, rows, cols = mixed.shape
    group = max(1, 128 // cols)
    total = None
    for n in range(0, members, group):
        part = jnp.concatenate([mixed[n + g] for g in range(group)], axis=1) if group > 1 else mixed[n]
        at = slice(n * cols, (n + group) * cols)
        block = raw[:, at].astype(F32) + part.astype(F32)
        resid[:, at] = block
        squares = jnp.sum(block * block, axis=1, keepdims=True)
        total = squares if total is None else total + squares
    scale = lax.rsqrt(total / (members * cols) + 1e-06)
    ffn[...] = (resid[...] * scale * gain[...]).astype(BF16)
    share = mine.shape[0]
    me = lax.axis_index("ep")
    for j in range(share):
        mine[j : j + 1] = resid[pl.ds(me * share + j, 1)]


def join_kernel(own, other, out):
    share = out.shape[1]
    both = own[...].astype(F32) + other[...].astype(F32)
    for e in range(out.shape[0]):
        out[e] = both[e * share : (e + 1) * share].astype(BF16)


def share_kernel(tokens, out):
    share = out.shape[1]
    me = lax.axis_index("tp")
    values = tokens[...].astype(F32)
    mine = jnp.where(me == 0, values[0:share], values[share:]).astype(BF16)
    for e in range(out.shape[0]):
        out[e] = mine


def gates_kernel(
    tokens, gain, w_in, w_forget, bias, stab, ids, weights, after, stab_out, decay, inweight, floor, route
):
    normed = rms_scale(tokens[...].astype(F32), gain[...]).astype(BF16)
    in_pre = product_t(normed, w_in[...])
    old = jax.nn.log_sigmoid(product_t(normed, w_forget[...]) + bias[...]) + stab[...]
    new = jnp.maximum(old, in_pre)
    stab_out[...] = new
    decay[...] = jnp.exp(old - new)
    inweight[...] = jnp.exp(in_pre - new)
    floor[...] = jnp.exp(-new)
    share, experts = route.shape
    seqs = ids.shape[1]
    label = lax.broadcasted_iota(jnp.int32, (seqs, experts), 1)
    same = lax.broadcasted_iota(jnp.int32, (seqs, seqs), 0) == lax.broadcasted_iota(jnp.int32, (seqs, seqs), 1)

    def column(row):
        return jnp.sum(jnp.where(same, row, 0.0), axis=1, keepdims=True)

    dense = jnp.zeros(label.shape, F32)
    for k in range(ids.shape[0]):
        chosen = column(ids[k : k + 1].astype(F32)).astype(jnp.int32)
        dense = dense + jnp.where(chosen == label, column(weights[k : k + 1]), 0.0)
    route[...] = jnp.where(lax.axis_index("tp") == 0, dense[0:share], dense[share:])


def finish_kernel(terms, route, resid, out):
    total = resid[...]
    for e in range(terms.shape[0]):
        total = total + route[:, e : e + 1] * terms[e].astype(F32)
    out[...] = total.astype(BF16)


def merge_kernel(mine, other, out):
    share = mine.shape[0]
    first = lax.axis_index("tp") == 0
    a, b = mine[...].astype(F32), other[...].astype(F32)
    out[0:share] = jnp.where(first, a, b).astype(BF16)
    out[share:] = jnp.where(first, b, a).astype(BF16)


def body(
    tokens,
    memory,
    normalizer,
    stabilizer,
    norm_gain,
    w_query,
    w_key,
    w_value,
    w_outgate,
    w_input,
    w_forget,
    forget_bias,
    w_out,
    ffn_gain,
    w_gate,
    w_up,
    w_down,
    expert_ids,
    route_weights,
):
    n_ep = lax.axis_size("ep")
    n_tp = lax.axis_size("tp")
    assert n_tp == 2
    swap = [(0, 1), (1, 0)]
    seqs, width = tokens.shape
    share = seqs // n_tp
    half = n_ep * share
    heads, key_size, value_size = (memory.shape[1], memory.shape[2], memory.shape[3])
    value_width = heads * value_size
    key_piece = w_query.shape[2]
    value_piece = w_value.shape[2]
    narrow = heads * key_piece
    broad = heads * value_piece
    total = 2 * narrow + 2 * broad

    copies = call(share_kernel, shape((n_ep, share, width), BF16), [VMEM], [], [tokens], "share", flops=LONG)
    gathered = to_all(copies)
    gathered_other = lax.ppermute(gathered, "tp", swap)
    raw_own, normed_own = call(
        front_kernel,
        (shape((half, width), BF16),) * 2,
        [VMEM] * 2,
        [],
        [gathered, norm_gain.reshape(1, width)],
        "front",
    )
    n_experts = n_ep * w_gate.shape[0]
    stab_next, decay, inweight, floor, route = call(
        gates_kernel,
        (shape((seqs, heads), F32),) * 4 + (shape((share, n_experts), F32),),
        [VMEM] * 8 + [ANY],
        [],
        [
            tokens,
            norm_gain.reshape(1, width),
            w_input.T,
            w_forget.T,
            forget_bias.reshape(1, heads),
            stabilizer,
            expert_ids.T,
            route_weights.T,
            normed_own,
        ],
        "gates",
    )
    columns = [jnp.transpose(w, (1, 2, 0)).reshape(-1, width) for w in (w_query, w_key, w_value, w_outgate)]
    projected = call(
        functools.partial(project_kernel, seqs=seqs),
        shape((n_ep, seqs, total), BF16),
        [VMEM] * 7 + [ANY],
        [pltpu.VMEM((2 * half, width), BF16)],
        [normed_own, gathered_other, norm_gain.reshape(1, width), *columns, route],
        "project",
        flops=LONG,
    )
    n_cells = seqs * heads
    pieces = to_all(projected)

    hidden, norm_next, key, value = call(
        functools.partial(readout_kernel, piece=(key_piece, value_piece)),
        (
            pltpu.HBM((n_ep, seqs, value_width), BF16),
            pltpu.HBM(normalizer.shape, F32),
            shape((heads * 8, key_size), F32),
            shape((seqs, value_width), F32),
        ),
        [VMEM] * 6,
        [
            pltpu.VMEM((seqs, value_width), F32),
            pltpu.VMEM((seqs, value_width), BF16),
            pltpu.VMEM(normalizer.shape, F32),
            pltpu.SemaphoreType.DMA((n_ep,)),
            pltpu.SemaphoreType.DMA((1,)),
        ],
        [pieces, decay, inweight, floor, normalizer, memory],
        "readout",
        flops=2 * memory.size,
        outs=(HBM, HBM, VMEM, VMEM),
    )
    hidden_all = to_all(hidden).reshape(n_ep * seqs, value_width)
    memory_next, w_out_near = call(
        update_kernel,
        (shape(memory.shape, F32), pltpu.VMEM(w_out.shape, BF16)),
        [VMEM] * 4 + [HBM] * 2,
        [
            pltpu.VMEM((n_cells, key_size, value_size), F32),
            pltpu.SemaphoreType.DMA((n_cells,)),
            pltpu.SemaphoreType.DMA((n_cells,)),
            pltpu.SemaphoreType.DMA((1,)),
        ],
        [key, value, decay, inweight, w_out, memory],
        "update",
        flops=10**8,
        outs=(HBM, VMEM),
    )

    own_term, other_term = call(
        functools.partial(output_kernel, seqs=seqs),
        (shape((half, w_out.shape[1]), BF16),) * 2,
        [VMEM, FAST],
        [],
        [hidden_all, w_out_near],
        "output",
        flops=LONG,
    )
    mixed = (own_term.astype(F32) + lax.ppermute(other_term, "tp", swap).astype(F32)).astype(BF16)
    mixed_all = to_all(jnp.broadcast_to(mixed[None], (n_ep,) + mixed.shape))

    ffn_own, resid_mine = call(
        resid_kernel,
        (shape((half, width), BF16), shape((share, width), F32)),
        [VMEM] * 3,
        [pltpu.VMEM((half, width), F32)],
        [raw_own, mixed_all, ffn_gain.reshape(1, width)],
        "resid",
    )
    ffn_other = lax.ppermute(ffn_own, "tp", swap)
    units = w_gate.shape[2]
    act_own, down_other = call(
        expert_kernel,
        (shape((half, units), BF16), shape((half, width), BF16)),
        [VMEM] * 5,
        [],
        [ffn_own, ffn_other, w_gate, w_up, w_down],
        "experts",
        flops=2 * 3 * half * width * units,
    )
    down_own = call(
        down_kernel, shape((half, width), BF16), [VMEM] * 2, [], [act_own, w_down], "down", flops=10**7
    )
    summed = call(
        join_kernel,
        shape((n_ep, share, width), BF16),
        [VMEM] * 2,
        [],
        [down_own, lax.ppermute(down_other, "tp", swap)],
        "join",
    )
    by_expert = to_all(summed)

    out_mine = call(
        finish_kernel, shape((share, width), BF16), [VMEM] * 3, [], [by_expert, route, resid_mine], "finish"
    )
    out = call(
        merge_kernel,
        shape((seqs, width), BF16),
        [VMEM] * 2,
        [],
        [out_mine, lax.ppermute(out_mine, "tp", swap)],
        "merge",
    )
    return (out, memory_next, norm_next, stab_next)


def solution(mesh):
    return jax.shard_map(
        body,
        mesh=mesh,
        in_specs=(
            P("ep", None),
            P("ep", "tp", None, None),
            P("ep", "tp", None),
            P("ep", "tp"),
            P(),
            P(None, "tp", "ep"),
            P(None, "tp", "ep"),
            P(None, "tp", "ep"),
            P(None, "tp", "ep"),
            P(None, "tp"),
            P(None, "tp"),
            P("tp"),
            P("tp", "ep"),
            P(),
            P("ep", None, "tp"),
            P("ep", None, "tp"),
            P("ep", "tp", None),
            P("ep", None),
            P("ep", None),
        ),
        out_specs=(P("ep", None), P("ep", "tp", None, None), P("ep", "tp", None), P("ep", "tp")),
        check_vma=False,
    )
```
